32 devices in a mesh: ep: 8 (over z, core), tp: 4 (over y, x).
Axes of the slice: x: 2, y: 2, z: 4, core: 2. Of those that a mesh axis runs over, the one named last changes fastest.
Arguments:
- tokens: bfloat16 [128, 2048], P('ep'), may hold values from -6 to 6
- attn_gain: float32 [2048], replicated, may hold values from 0.1 to 1.9
- query_weight: bfloat16 [2048, 2048], P('ep', 'tp'), may hold values from -0.125 to 0.125
- key_weight: bfloat16 [2048, 2048], P('ep', 'tp'), may hold values from -0.125 to 0.125
- value_weight: bfloat16 [2048, 2048], P('ep', 'tp'), may hold values from -0.125 to 0.125
- forget_weight: bfloat16 [2048, 16], P(None, 'tp'), may hold values from -0.125 to 0.125
- forget_bias: float32 [16], P('tp'), may hold values from -1 to 2
- cache_keys: bfloat16 [128, 16, 384, 128], P('ep', 'tp'), may hold values from -240 to 240
- cache_values: bfloat16 [128, 16, 384, 128], P('ep', 'tp'), may hold values from -6 to 6
- cache_gates: float32 [128, 16, 384], P('ep', 'tp'), may hold values from -768 to 0, as said below
- lengths: int32 [128], P('ep'), may hold values from 1 to 384
- output_weight: bfloat16 [2048, 2048], P('tp', 'ep'), may hold values from -0.125 to 0.125
- ffn_gain: float32 [2048], replicated, may hold values from 0.1 to 1.9
- dense_gate_proj: bfloat16 [2048, 2048], P('ep', 'tp'), may hold values from -0.125 to 0.125
- dense_up_proj: bfloat16 [2048, 2048], P('ep', 'tp'), may hold values from -0.125 to 0.125
- dense_down_proj: bfloat16 [2048, 2048], P('tp', 'ep'), may hold values from -0.125 to 0.125
- dense_mix: bfloat16 [2048], replicated, may hold values from -0.125 to 0.125
- expert_ids: int32 [128, 2], P('ep'), may hold values from 0 to 7, as said below
- group_prob: float32 [128], P('ep'), may hold values from 0.25 to 1
- pair_prob: float32 [128, 2], P('ep'), may hold values from 0.05 to 1
- expert_gate: bfloat16 [8, 2048, 2048], P('ep', None, 'tp'), may hold values from -0.125 to 0.125
- expert_up: bfloat16 [8, 2048, 2048], P('ep', None, 'tp'), may hold values from -0.125 to 0.125
- expert_down: bfloat16 [8, 2048, 2048], P('ep', 'tp'), may hold values from -0.125 to 0.125
Outputs:
- mixed_out: bfloat16 [128, 2048], P('ep')
The draws below stay inside these ranges and needn't reach their ends.
Inputs may be any that keep to these rules, and one draw needn't show every extreme that they name: `expert_ids`: each row names two different experts of one group, the groups being 4 runs of consecutive ids. In each aligned block of 16 rows (the rows of one index of ep) no expert is named more than 8 times, and some expert exactly 8 times. `cache_gates`: along positions the values never rise.
All inputs are finite; a program needn't handle non-finite values.
Results may differ from the reference program's by a relative error of at most 0.014.
Values may be sent and summed in bfloat16 or wider, within the bound.
A program may use at most 64 MiB of HBM per device.

```python
import math
import jax
import jax.numpy as jnp
from jax import lax

D = 2048
HEAD_TOTAL = 16
HEAD = 128
FF_D = 2048
FF_E = 2048
GROUPS = 4
SEQ_DEV = 16
CACHED_LENGTH = 384
SEQUENCE_TOTAL = 128
EXPERTS = 8
CAP = 8
N_EP = 8


def draw_cache_keys(key, part):
    first_key = jax.random.fold_in(key, 0)
    base = jnp.clip(jax.random.normal(first_key, (SEQUENCE_TOTAL, HEAD_TOTAL, CACHED_LENGTH, HEAD), jnp.float32), -6.0, 6.0)
    return base.astype(jnp.bfloat16)


def draw_cache_gates(key, part):
    every_key = jax.random.split(key, 7)
    fast_share = 0.5
    fast_heads = jax.random.uniform(every_key[0], (1, HEAD_TOTAL, 1), jnp.float32) < fast_share
    slow_rate = jnp.exp(jax.random.uniform(every_key[1], (SEQUENCE_TOTAL, HEAD_TOTAL, 1), jnp.float32, math.log(0.3), math.log(2.0))) / CACHED_LENGTH
    fast_rate = jnp.exp(jax.random.uniform(every_key[2], (SEQUENCE_TOTAL, HEAD_TOTAL, 1), jnp.float32, math.log(1.0 / 100.0), math.log(1.0 / 30.0)))
    seq_factor = jnp.exp(jax.random.uniform(every_key[3], (SEQUENCE_TOTAL, 1, 1), jnp.float32, math.log(0.5), math.log(2.0)))
    coarse_scores = jax.random.uniform(every_key[4], (SEQUENCE_TOTAL, HEAD_TOTAL, CACHED_LENGTH), jnp.float32, 0.3, 1.7)
    decay_rate = jnp.where(fast_heads, fast_rate, slow_rate) * seq_factor
    spike_mask = jax.random.uniform(every_key[5], (SEQUENCE_TOTAL, HEAD_TOTAL, CACHED_LENGTH), jnp.float32) < 3.0 / CACHED_LENGTH
    spike_length = jnp.log(jax.random.uniform(every_key[6], (SEQUENCE_TOTAL, HEAD_TOTAL, CACHED_LENGTH), jnp.float32, 0.5, 0.8))
    gate_logs = -decay_rate * coarse_scores + jnp.where(spike_mask, spike_length, 0.0)
    return jnp.cumsum(gate_logs, axis=-1).astype(jnp.float32)


def draw_expert_ids(key, part):
    group_width = EXPERTS // GROUPS
    pair_count = CAP * group_width // 2

    def one_block(block_key):
        every_key = jax.random.split(block_key, 4)
        heavy = jax.random.randint(every_key[0], (), 0, GROUPS)
        perm_keys = jax.random.split(every_key[1], GROUPS * CAP)
        orders = jax.vmap(lambda perm_key: jax.random.permutation(perm_key, group_width))(perm_keys)
        orders = orders.reshape(GROUPS, CAP * group_width).astype(jnp.int32)
        orders = orders + (jnp.arange(GROUPS, dtype=jnp.int32) * group_width)[:, None]
        pair_ids = orders.reshape(GROUPS * pair_count, 2)
        ranking = jax.random.permutation(every_key[2], GROUPS * pair_count).astype(jnp.int32)
        group_of = jnp.arange(GROUPS * pair_count, dtype=jnp.int32) // pair_count
        priority = jnp.where(group_of == heavy, 0, GROUPS * pair_count) + ranking
        chosen = jnp.argsort(priority, stable=True)[:SEQ_DEV]
        picked = pair_ids[chosen]
        shuffle = jax.random.permutation(every_key[3], SEQ_DEV)
        return picked[shuffle]
    block_keys = jax.random.split(key, SEQUENCE_TOTAL // SEQ_DEV)
    return jax.vmap(one_block)(block_keys).reshape(SEQUENCE_TOTAL, 2).astype(jnp.int32)


def with_ends(values, key, smallest, high):
    spot = [jax.random.randint(jax.random.fold_in(key, axis), (), 0, length) for axis, length in enumerate(values.shape)]
    main_axis = values.shape.index(max(values.shape))
    beside = spot[:main_axis] + [(spot[main_axis] + 1) % values.shape[main_axis]] + spot[main_axis + 1:]
    return values.at[tuple(spot)].set(smallest).at[tuple(beside)].set(high)


def shard_levels(key, shape, shards, low, high):
    factor_of = 1.0
    for axis_at, parts in shards:
        draws = jax.random.uniform(jax.random.fold_in(jax.random.fold_in(key, 6), axis_at), (parts,), jnp.float32, low / len(shards), high / len(shards))
        factor_of = factor_of * jnp.repeat(jnp.exp(draws), shape[axis_at] // parts).reshape((-1,) + (1,) * (len(shape) - 1 - axis_at))
    return factor_of


def gaussian(key, dims, scale, bound, shards=(), held_as=jnp.bfloat16):
    array = scale * jax.random.normal(key, dims, jnp.float32)
    if shards:
        array = array * shard_levels(key, dims, shards, -0.22, 0.18)
    return jnp.clip(array, -bound, bound).astype(held_as)


def setup_inputs(seed: int = 0) -> dict:
    seeds = jax.random.split(jax.random.key(seed), 24)
    return {
        "tokens": gaussian(seeds[0], (SEQUENCE_TOTAL, D), 1.0, 6.0, ((0, 8),)),
        "attn_gain": jnp.clip(1.0 + 0.18 * jax.random.normal(seeds[1], (D,), jnp.float32), 0.1, 1.9),
        "query_weight": gaussian(seeds[2], (D, HEAD_TOTAL * HEAD), D ** -0.5, 0.125, ((0, 8), (1, 4))),
        "key_weight": gaussian(seeds[3], (D, HEAD_TOTAL * HEAD), D ** -0.5, 0.125, ((0, 8), (1, 4))),
        "value_weight": gaussian(seeds[4], (D, HEAD_TOTAL * HEAD), D ** -0.5, 0.125, ((0, 8), (1, 4))),
        "forget_weight": gaussian(seeds[5], (D, HEAD_TOTAL), D ** -0.5, 0.125, ((1, 4),)),
        "forget_bias": jnp.clip(-1.0 + 3.0 * jax.random.uniform(seeds[6], (HEAD_TOTAL,), jnp.float32) ** shard_levels(seeds[6], (HEAD_TOTAL,), ((0, 4),), -0.2, 0.2), -1.0, 2.0),
        "cache_keys": draw_cache_keys(jax.random.fold_in(seeds[23], 71), 0),
        "cache_values": gaussian(seeds[8], (SEQUENCE_TOTAL, HEAD_TOTAL, CACHED_LENGTH, HEAD), 1.0, 6.0, ((0, 8), (1, 4))),
        "cache_gates": draw_cache_gates(jax.random.fold_in(seeds[23], 71), 0),
        "lengths": with_ends(jax.random.randint(seeds[10], (SEQUENCE_TOTAL,), 1, CACHED_LENGTH + 1), jax.random.fold_in(seeds[10], 1), 1, CACHED_LENGTH).astype(jnp.int32),
        "output_weight": gaussian(seeds[11], (HEAD_TOTAL * HEAD, D), (HEAD_TOTAL * HEAD) ** -0.5, 0.125, ((0, 4), (1, 8))),
        "ffn_gain": jnp.clip(1.0 + 0.18 * jax.random.normal(seeds[12], (D,), jnp.float32), 0.1, 1.9),
        "dense_gate_proj": gaussian(seeds[13], (D, FF_D), D ** -0.5, 0.125, ((0, 8), (1, 4))),
        "dense_up_proj": gaussian(seeds[14], (D, FF_D), D ** -0.5, 0.125, ((0, 8), (1, 4))),
        "dense_down_proj": gaussian(seeds[15], (FF_D, D), FF_D ** -0.5, 0.125, ((0, 4), (1, 8))),
        "dense_mix": gaussian(seeds[16], (D,), D ** -0.5, 0.125),
        "expert_ids": draw_expert_ids(jax.random.fold_in(seeds[23], 71), 0),
        "group_prob": jnp.clip(jnp.exp(math.log(1.0) - 1.3862944 * jax.random.uniform(seeds[18], (SEQUENCE_TOTAL,), jnp.float32) ** shard_levels(seeds[18], (SEQUENCE_TOTAL,), ((0, 8),), -0.2, 0.2)), 0.25, 1.0),
        "pair_prob": jnp.clip(0.05 + 0.95 * jax.random.uniform(seeds[19], (SEQUENCE_TOTAL, 2), jnp.float32) ** shard_levels(seeds[19], (SEQUENCE_TOTAL, 2), ((0, 8),), -0.2, 0.2), 0.05, 1.0),
        "expert_gate": gaussian(seeds[20], (EXPERTS, D, FF_E), D ** -0.5, 0.125, ((0, 8), (2, 4))),
        "expert_up": gaussian(seeds[21], (EXPERTS, D, FF_E), D ** -0.5, 0.125, ((0, 8), (2, 4))),
        "expert_down": gaussian(seeds[22], (EXPERTS, FF_E, D), FF_E ** -0.5, 0.125, ((0, 8), (1, 4))),
    }


EPSILON = 1e-06

def rms_scale(values, norm_gain):
    widened = values.astype(jnp.float32)
    return widened * lax.rsqrt(lax.optimization_barrier(jnp.mean(widened * widened, axis=-1, keepdims=True)) + EPSILON) * norm_gain

def attend(members):
    queries, keys_new, values_new, key_cache, value_cache, gate_cache, lengths, log_forget = members
    cache_span = key_cache.shape[2]
    score_scale = 1.0 / math.sqrt(key_cache.shape[3])
    positions = jnp.arange(cache_span, dtype=jnp.int32)
    live_mask = positions[None, :] < lengths[:, None]
    last_mask = positions[None, :] == lengths[:, None] - 1
    last_gate = lax.optimization_barrier(jnp.sum(jnp.where(last_mask[:, None, :], gate_cache, 0.0), axis=-1))
    gate_now = last_gate + log_forget
    scores = jnp.einsum('shd,shpd->shp', queries.astype(jnp.float32), key_cache.astype(jnp.float32)) * score_scale
    scores = scores + gate_now[:, :, None] - gate_cache
    scores = jnp.where(live_mask[:, None, :], scores, -jnp.inf)
    own_score = lax.optimization_barrier(jnp.sum(queries.astype(jnp.float32) * keys_new.astype(jnp.float32), axis=-1)) * score_scale
    row_top = jnp.maximum(lax.optimization_barrier(jnp.max(scores, axis=-1)), own_score)
    raised = jnp.exp(scores - row_top[:, :, None])
    own_raised = jnp.exp(own_score - row_top)
    totals = lax.optimization_barrier(jnp.sum(raised, axis=-1)) + own_raised
    weights_low = (raised / totals[:, :, None]).astype(jnp.bfloat16)
    own_prob = (own_raised / totals).astype(jnp.bfloat16)
    attended = jnp.einsum('shp,shpd->shd', weights_low.astype(jnp.float32), value_cache.astype(jnp.float32))
    attended = attended + own_prob.astype(jnp.float32)[:, :, None] * values_new.astype(jnp.float32)
    return attended.astype(jnp.bfloat16)

def by_block(array_in):
    return array_in.reshape((N_EP, array_in.shape[0] // N_EP) + array_in.shape[1:])

def reference(tokens, attn_gain, query_weight, key_weight, value_weight, forget_weight, forget_bias, cache_keys, cache_values, cache_gates, lengths, output_weight, ffn_gain, dense_gate_proj, dense_up_proj, dense_down_proj, dense_mix, expert_ids, group_prob, pair_prob, expert_gate, expert_up, expert_down):
    seq_count = tokens.shape[0]
    normed = rms_scale(tokens, attn_gain).astype(jnp.bfloat16)
    queries = jnp.dot(normed, query_weight, preferred_element_type=jnp.float32).astype(jnp.bfloat16)
    keys_new = jnp.dot(normed, key_weight, preferred_element_type=jnp.float32).astype(jnp.bfloat16)
    values_new = jnp.dot(normed, value_weight, preferred_element_type=jnp.float32).astype(jnp.bfloat16)
    queries = queries.reshape(seq_count, HEAD_TOTAL, HEAD)
    keys_new = keys_new.reshape(seq_count, HEAD_TOTAL, HEAD)
    values_new = values_new.reshape(seq_count, HEAD_TOTAL, HEAD)
    log_forget = jax.nn.log_sigmoid(jnp.dot(normed, forget_weight, preferred_element_type=jnp.float32) + forget_bias)
    members = tuple((by_block(item) for item in (queries, keys_new, values_new, cache_keys, cache_values, cache_gates, lengths, log_forget)))
    attended = lax.map(attend, members).reshape(seq_count, HEAD_TOTAL * HEAD)
    residual = (tokens.astype(jnp.float32) + jnp.dot(attended, output_weight, preferred_element_type=jnp.float32)).astype(jnp.bfloat16)
    ffn_in = rms_scale(residual, ffn_gain).astype(jnp.bfloat16)
    dense_gate_part = jnp.dot(ffn_in, dense_gate_proj, preferred_element_type=jnp.float32)
    dense_up_part = jnp.dot(ffn_in, dense_up_proj, preferred_element_type=jnp.float32)
    dense_hidden = (jax.nn.silu(dense_gate_part) * dense_up_part).astype(jnp.bfloat16)
    dense_total = jnp.dot(dense_hidden, dense_down_proj, preferred_element_type=jnp.float32)
    mix = jax.nn.sigmoid(jnp.dot(ffn_in, dense_mix, preferred_element_type=jnp.float32))
    routes = group_prob[:, None] * pair_prob / lax.optimization_barrier(jnp.sum(pair_prob, axis=1, keepdims=True))
    most_rows = CAP * N_EP

    def one_expert(accum, expert_index):
        hit_mask = expert_ids == expert_index
        row_weight = lax.optimization_barrier(jnp.sum(jnp.where(hit_mask, routes, 0.0), axis=1))
        any_hit = lax.optimization_barrier(jnp.sum(hit_mask.astype(jnp.int32), axis=1)) > 0
        chosen = jnp.nonzero(any_hit, size=most_rows, fill_value=0)[0].astype(jnp.int32)
        valid_rows = jnp.arange(most_rows, dtype=jnp.int32) < jnp.sum(any_hit.astype(jnp.int32))
        row_data = ffn_in[chosen]
        gate_part = jnp.dot(row_data, expert_gate[expert_index], preferred_element_type=jnp.float32)
        up_part = jnp.dot(row_data, expert_up[expert_index], preferred_element_type=jnp.float32)
        expert_hidden = (jax.nn.silu(gate_part) * up_part).astype(jnp.bfloat16)
        expert_out = jnp.dot(expert_hidden, expert_down[expert_index], preferred_element_type=jnp.float32)
        weight_rows = jnp.where(valid_rows, row_weight[chosen], 0.0)
        return (accum.at[chosen].add(weight_rows[:, None] * expert_out), None)
    expert_sum, _ = lax.scan(one_expert, jnp.zeros((seq_count, D), jnp.float32), jnp.arange(EXPERTS, dtype=jnp.int32))
    result = residual.astype(jnp.float32) + expert_sum + mix[:, None] * dense_total
    return result.astype(jnp.bfloat16)
```

```python
import functools
import math

import jax
import jax.numpy as jnp
from jax import lax
from jax.experimental import pallas as pl
from jax.experimental.pallas import tpu as pltpu
from jax.sharding import PartitionSpec as P

EPSILON = 1e-06


def rms_scale(values, norm_gain):
    widened = values.astype(jnp.float32)
    return (
        widened
        * lax.rsqrt(jnp.mean(widened * widened, axis=-1, keepdims=True) + EPSILON)
        * norm_gain
    )


MESH = pl.DeviceIdType.MESH
F32 = jnp.float32
BF16 = jnp.bfloat16


def fan_out(axis, count, me, source_of, landing, send_sem, recv_sem, slot=None):
    copies = []
    place = me if slot is None else slot(me)
    for step in range(1, count):
        target = lax.rem(me + step, count)
        copy = pltpu.make_async_remote_copy(
            src_ref=source_of(target),
            dst_ref=landing.at[place],
            send_sem=send_sem.at[step],
            recv_sem=recv_sem.at[me],
            device_id={axis: target},
            device_id_type=MESH,
        )
        copy.start()
        copies.append(copy)
    return copies


def collect(axis, count, me, landing, send_sem, recv_sem, slot=None):
    for step in range(1, count):
        source = lax.rem(me + count - step, count)
        place = source if slot is None else slot(source)
        pltpu.make_async_remote_copy(
            src_ref=landing.at[place],
            dst_ref=landing.at[place],
            send_sem=send_sem.at[step],
            recv_sem=recv_sem.at[source],
            device_id={axis: source},
            device_id_type=MESH,
        ).wait_recv()


def spread_rows(axis_ep, axis_tp, n_ep, n_tp, me_ep, me_tp, held, landing, send_sem, recv_sem):
    ratio = n_ep // n_tp
    for part in range(ratio):
        target_ep = me_tp * ratio + part
        for step in range(n_tp):
            target_tp = lax.rem(me_tp + step, n_tp)

            def send():
                pltpu.make_async_remote_copy(
                    src_ref=held.at[part],
                    dst_ref=landing.at[me_ep],
                    send_sem=send_sem.at[part * n_tp + step],
                    recv_sem=recv_sem.at[me_ep],
                    device_id={axis_ep: target_ep, axis_tp: target_tp},
                    device_id_type=MESH,
                ).start()

            if step == 0:
                pl.when(target_ep != me_ep)(send)

                @pl.when(target_ep == me_ep)
                def _():
                    landing[me_ep] = held[part]
            else:
                send()


def spread_wait(axis_ep, axis_tp, n_ep, n_tp, me_ep, me_tp, held, landing, send_sem, recv_sem):
    ratio = n_ep // n_tp
    own_tp = me_ep // ratio
    for step in range(n_ep):
        source = lax.rem(me_ep + n_ep - step, n_ep)

        def arrive():
            pltpu.make_async_remote_copy(
                src_ref=landing.at[source],
                dst_ref=landing.at[source],
                send_sem=send_sem.at[0],
                recv_sem=recv_sem.at[source],
                device_id={axis_ep: source, axis_tp: own_tp},
                device_id_type=MESH,
            ).wait_recv()

        if step == 0:
            pl.when(own_tp != me_tp)(arrive)
        else:
            arrive()


def spread_sent(axis_ep, axis_tp, n_ep, n_tp, me_ep, me_tp, held, landing, send_sem, recv_sem):
    ratio = n_ep // n_tp
    for part in range(ratio):
        target_ep = me_tp * ratio + part
        for step in range(n_tp):
            target_tp = lax.rem(me_tp + step, n_tp)

            def sent():
                pltpu.make_async_remote_copy(
                    src_ref=held.at[part],
                    dst_ref=landing.at[me_ep],
                    send_sem=send_sem.at[part * n_tp + step],
                    recv_sem=recv_sem.at[me_ep],
                    device_id={axis_ep: target_ep, axis_tp: target_tp},
                    device_id_type=MESH,
                ).wait_send()

            if step == 0:
                pl.when(target_ep != me_ep)(sent)
            else:
                sent()


def total_of(ref, count):
    total = ref[0].astype(F32)
    for index in range(1, count):
        total = total + ref[index].astype(F32)
    return total


def dot32(left, right):
    return jnp.dot(left, right, preferred_element_type=F32)


def chip_order(index, half):
    return lax.rem(index, 2) * half + index // 2


def pair_copy(axis, me, source, landing, send_sem, recv_sem, slot):
    return pltpu.make_async_remote_copy(
        src_ref=source,
        dst_ref=landing,
        send_sem=send_sem.at[slot],
        recv_sem=recv_sem.at[slot],
        device_id={axis: me + 1 - 2 * lax.rem(me, 2)},
        device_id_type=MESH,
    )


def chip_fan(axis, half, me, held, landing, send_sem, recv_sem):
    chip, core = me // 2, lax.rem(me, 2)
    copies = []
    for step in range(1, half):
        target = lax.rem(chip + step, half)
        copy = pltpu.make_async_remote_copy(
            src_ref=held.at[target],
            dst_ref=landing.at[chip],
            send_sem=send_sem.at[step],
            recv_sem=recv_sem.at[chip],
            device_id={axis: target * 2 + core},
            device_id_type=MESH,
        )
        copy.start()
        copies.append(copy)
    landing[chip] = held[chip]
    return copies


def chip_collect(axis, half, me, landing, send_sem, recv_sem):
    chip, core = me // 2, lax.rem(me, 2)
    for step in range(1, half):
        source = lax.rem(chip + half - step, half)
        pltpu.make_async_remote_copy(
            src_ref=landing.at[source],
            dst_ref=landing.at[source],
            send_sem=send_sem.at[step],
            recv_sem=recv_sem.at[source],
            device_id={axis: source * 2 + core},
            device_id_type=MESH,
        ).wait_recv()


def pick(one_hot, held):
    return lax.dot_general(
        one_hot, held, (((0,), (0,)), ((), ())), preferred_element_type=F32
    )


def slot_tables(expert_ids, group_prob, pair_prob, experts, slots):
    rows = expert_ids.shape[1]
    ids = expert_ids[...]
    row_at = lax.broadcasted_iota(jnp.int32, (rows, rows), 0)
    row_to = lax.broadcasted_iota(jnp.int32, (rows, rows), 1)
    expert_at = lax.broadcasted_iota(jnp.int32, (experts, rows), 0)
    first = ids[0:1, :] == expert_at
    second = ids[1:2, :] == expert_at
    hits = (first | second).astype(F32).astype(BF16)
    earlier = (row_at < row_to).astype(F32).astype(BF16)
    ranks = dot32(hits, earlier)
    slot_at = lax.broadcasted_iota(jnp.int32, (slots, rows), 0).astype(F32)
    tables = []
    for chosen in (first, second):
        place = jnp.where(chosen, ranks, -1.0)
        tables.append(
            jnp.concatenate(
                [
                    (place[expert : expert + 1, :] == slot_at).astype(F32)
                    for expert in range(experts)
                ],
                axis=0,
            )
        )
    probs = pair_prob[...]
    shares = group_prob[...] * probs / (probs[0:1, :] + probs[1:2, :])
    columns = [
        jnp.sum(jnp.where(row_at == row_to, shares[k : k + 1, :], 0.0), axis=-1, keepdims=True)
        for k in range(2)
    ]
    both = (tables[0] + tables[1]).astype(BF16)
    return tables[0].astype(BF16), tables[1].astype(BF16), both, columns[0], columns[1]


def layer_kernel(
    n_ep,
    n_tp,
    forget_bias,
    lengths,
    tokens,
    attn_gain,
    forget_rows,
    gates,
    gain,
    gain_parts,
    dense_mix,
    expert_ids,
    group_prob,
    pair_prob,
    query_weight,
    key_weight,
    value_weight,
    keys,
    values,
    output_weight,
    dense_gate,
    dense_up,
    expert_gate,
    expert_up,
    expert_down,
    dense_down,
    out,
    query_weight_held,
    key_weight_held,
    value_weight_held,
    keys_held,
    values_held,
    output_weight_held,
    dense_gate_held,
    dense_up_held,
    expert_gate_held,
    expert_up_held,
    expert_down_held,
    dense_down_held,
    load_sem,
    norm_send,
    norm_land,
    norm_ss,
    norm_rs,
    part_send,
    part_land,
    part_ss,
    part_rs,
    score_send,
    score_land,
    score_ss,
    score_rs,
    value_send,
    value_land,
    value_ss,
    value_rs,
    query_rows,
    key_rows,
    value_rows,
    forget_logs,
    scores,
    mixed,
    attended,
    full,
    att_land,
    att_ss,
    att_rs,
    head_send,
    head_land,
    head_ss,
    head_rs,
    mix_send,
    mix_land,
    mix_ss,
    mix_rs,
    token_send,
    token_land,
    token_ss,
    token_rs,
    share_land,
    share_ss,
    share_rs,
    slot_send,
    slot_land,
    slot_ss,
    slot_rs,
    pair_send,
    pair_land,
    pair_ss,
    pair_rs,
    dense_send,
    dense_land,
    dense_ss,
    dense_rs,
    expert_send,
    expert_land,
    expert_ss,
    expert_rs,
    back_send,
    back_land,
    back_ss,
    back_rs,
    hidden_send,
    hidden_land,
    hidden_ss,
    hidden_rs,
    down_send,
    down_land,
    down_ss,
    down_rs,
    tail_send,
    tail_land,
    tail_ss,
    tail_rs,
    route_send,
    route_land,
    route_ss,
    route_rs,
):
    me = lax.axis_index("ep")
    me_tp = lax.axis_index("tp")
    barrier = pltpu.get_barrier_semaphore()
    everyone = n_ep * n_tp
    place = me * n_tp + me_tp

    def greet(step, carry):
        other = lax.rem(place + step, everyone)
        pl.semaphore_signal(
            barrier,
            inc=1,
            device_id={"ep": other // n_tp, "tp": lax.rem(other, n_tp)},
            device_id_type=MESH,
        )
        return carry

    lax.fori_loop(1, everyone, greet, 0)
    sources = (query_weight, key_weight, value_weight, keys, values, output_weight, dense_gate, dense_up, expert_gate, expert_up, expert_down, dense_down)
    places = (query_weight_held, key_weight_held, value_weight_held, keys_held, values_held, output_weight_held, dense_gate_held, dense_up_held, expert_gate_held, expert_up_held, expert_down_held, dense_down_held)
    loads = [
        pltpu.make_async_copy(source, place, load_sem.at[index])
        for index, (source, place) in enumerate(zip(sources, places))
    ]
    for load in loads:
        load.start()
    rows, model = tokens.shape
    depth, hidden = query_weight.shape
    heads, span, size = keys.shape[1:]
    slots = slot_send.shape[1]
    group_rows = n_ep * rows // n_tp
    ratio = n_ep // n_tp
    half = n_ep // 2
    chip, core = me // 2, lax.rem(me, 2)
    grid = (n_ep, n_tp, me, me_tp)

    def order(index):
        return chip_order(index, half)

    normed = rms_scale(tokens[...], attn_gain[...])
    for index in range(n_ep):
        norm_send[index] = normed[:, index * depth : (index + 1) * depth].astype(BF16)
        token_send[index] = tokens[:, index * depth : (index + 1) * depth]
    pl.semaphore_wait(barrier, everyone - 1)

    sent = fan_out("ep", n_ep, me, lambda t: norm_send.at[t], norm_land, norm_ss, norm_rs, order)
    norm_land[order(me)] = norm_send[me]
    sent += fan_out("ep", n_ep, me, lambda t: token_send.at[t], token_land, token_ss, token_rs)
    token_land[me] = token_send[me]
    normed_wide = normed.astype(BF16).astype(F32)
    for head in range(heads):
        logit = forget_bias[0, head] + jnp.sum(
            normed_wide * forget_rows[head : head + 1, :].astype(F32), axis=-1, keepdims=True
        )
        forget_log = jnp.minimum(logit, 0.0) - jnp.log1p(jnp.exp(-jnp.abs(logit)))
        forget_logs[:, head, :] = jnp.broadcast_to(forget_log, (rows, size))
    collect("ep", n_ep, me, norm_land, norm_ss, norm_rs, order)
    joined = norm_land[...].reshape(n_ep * rows, depth)
    swaps = []
    for index, weight in enumerate((query_weight_held, key_weight_held, value_weight_held)):
        loads[index].wait()
        part_send[index] = dot32(joined, weight[...]).reshape(2, half, rows, hidden)
        swap = pair_copy(
            "ep", me, part_send.at[index, 1 - core], part_land.at[index], part_ss, part_rs, index
        )
        swap.start()
        swaps.append(swap)
    sent += swaps
    for index in range(2):
        swaps[index].wait_recv()
        score_send[index] = part_send[index, core] + part_land[index]
        sent += chip_fan(
            "ep",
            half,
            me,
            score_send.at[index],
            score_land.at[index],
            score_ss.at[index],
            score_rs.at[index],
        )
    swaps[2].wait_recv()
    value_send[...] = (part_send[2, core] + part_land[2]).astype(BF16)
    sent += chip_fan("ep", half, me, value_send, value_land, value_ss, value_rs)
    to_first, to_second, to_slots, first_route, second_route = slot_tables(
        expert_ids, group_prob, pair_prob, n_ep, slots
    )
    chip_collect("ep", half, me, score_land.at[0], score_ss.at[0], score_rs.at[0])
    summed = total_of(score_land.at[0], half).astype(BF16).astype(F32)
    for head in range(heads):
        query_rows[:, head, :] = summed[:, head * size : (head + 1) * size]

    scale = 1.0 / math.sqrt(size)
    loads[3].wait()
    loads[4].wait()

    def score_step(seq, carry):
        for head in range(heads):
            query = query_rows[seq, head : head + 1, :].astype(BF16)
            scores[seq, head : head + 1, :] = lax.dot_general(
                query,
                keys_held[seq, head],
                (((1,), (1,)), ((), ())),
                preferred_element_type=F32,
            )
        return carry

    lax.fori_loop(0, rows, score_step, 0, unroll=4)
    chip_collect("ep", half, me, score_land.at[1], score_ss.at[1], score_rs.at[1])
    summed = total_of(score_land.at[1], half).astype(BF16).astype(F32)
    for head in range(heads):
        key_rows[:, head, :] = summed[:, head * size : (head + 1) * size]
    positions = lax.broadcasted_iota(jnp.int32, (rows, heads, span), 2)
    sequences = lax.broadcasted_iota(jnp.int32, (rows, heads, size), 0)
    live_wide = jnp.zeros((rows, heads, size), jnp.int32)
    for seq in range(rows):
        live_wide = jnp.where(sequences == seq, lengths[0, seq], live_wide)
    lives = live_wide[:, :, 0:1]
    gate_all = gates[...]
    last_gate = jnp.sum(jnp.where(positions == lives - 1, gate_all, 0.0), axis=-1, keepdims=True)
    gate_now = last_gate + forget_logs[:, :, 0:1]
    score_all = scores[...] * scale + gate_now - gate_all
    score_all = jnp.where(positions < lives, score_all, -jnp.inf)
    own_score = jnp.sum(query_rows[...] * key_rows[...], axis=-1, keepdims=True) * scale
    row_top = jnp.maximum(jnp.max(score_all, axis=-1, keepdims=True), own_score)
    raised = jnp.exp(score_all - row_top)
    own_raised = jnp.exp(own_score - row_top)
    totals = jnp.sum(raised, axis=-1, keepdims=True) + own_raised
    scores[...] = raised / totals
    own_prob = (own_raised / totals).astype(BF16).astype(F32)

    def value_step(seq, carry):
        for head in range(heads):
            weight = scores[seq, head : head + 1, :].astype(BF16)
            mixed[seq, head : head + 1, :] = dot32(weight, values_held[seq, head])
        return carry

    lax.fori_loop(0, rows, value_step, 0, unroll=4)
    chip_collect("ep", half, me, value_land, value_ss, value_rs)
    value_sum = total_of(value_land, half).astype(BF16).astype(F32)
    for head in range(heads):
        value_rows[:, head, :] = value_sum[:, head * size : (head + 1) * size]
    mixed[...] = mixed[...] + own_prob * value_rows[...]
    for head in range(heads):
        attended[:, head * size : (head + 1) * size] = mixed[:, head, :].astype(BF16)

    sent += fan_out("ep", n_ep, me, lambda t: attended, att_land, att_ss, att_rs)
    att_land[me] = attended[...]
    collect("ep", n_ep, me, att_land, att_ss, att_rs)
    loads[5].wait()
    shares = dot32(att_land[...].reshape(n_ep * rows, hidden), output_weight_held[...])
    head_send[...] = shares.reshape(n_tp, group_rows, depth)
    sent += fan_out("tp", n_tp, me_tp, lambda t: head_send.at[t], head_land, head_ss, head_rs)
    head_land[me_tp] = head_send[me_tp]
    collect("tp", n_tp, me_tp, head_land, head_ss, head_rs)
    mix_send[...] = total_of(head_land, n_tp).reshape(ratio, rows, depth)
    spread_rows("ep", "tp", *grid, mix_send, mix_land, mix_ss, mix_rs)
    sent += fan_out("tp", n_tp, me_tp, lambda t: mix_send, share_land, share_ss, share_rs)
    share_land[me_tp] = mix_send[...]
    collect("ep", n_ep, me, token_land, token_ss, token_rs)
    collect("tp", n_tp, me_tp, share_land, share_ss, share_rs)

    shared = share_land[...].reshape(n_ep, rows, depth)
    residual_part = (token_land[...].astype(F32) + shared).astype(BF16)
    dense_rows = (residual_part.astype(F32) * gain_parts[me]).astype(BF16)
    dense_rows = dense_rows.reshape(n_ep * rows, depth)
    for index, weight in enumerate((dense_gate_held, dense_up_held)):
        loads[6 + index].wait()
        product = dot32(dense_rows, weight[...])
        for place in range(n_ep):
            pair_send[place % 2, place // 2, :, index * hidden : (index + 1) * hidden] = product[
                place * rows : (place + 1) * rows
            ]
    swap = pair_copy("ep", me, pair_send.at[1 - core], pair_land, pair_ss, pair_rs, 0)
    swap.start()
    swap.wait_recv()
    sent.append(swap)
    dense_send[...] = (pair_send[core] + pair_land[...]).astype(BF16)
    sent += chip_fan("ep", half, me, dense_send, dense_land, dense_ss, dense_rs)

    spread_wait("ep", "tp", *grid, mix_send, mix_land, mix_ss, mix_rs)
    for index in range(n_ep):
        full[:, index * depth : (index + 1) * depth] = mix_land[index]
    residual = (tokens[...].astype(F32) + full[...]).astype(BF16)
    residual_wide = residual.astype(F32)
    row_scale = lax.rsqrt(
        jnp.mean(residual_wide * residual_wide, axis=-1, keepdims=True) + EPSILON
    )
    ffn_in = (residual_wide * row_scale * gain[...]).astype(BF16)

    outbound = dot32(to_slots, ffn_in)
    for index in range(n_ep):
        slot_send[index] = outbound[index * slots : (index + 1) * slots].astype(BF16)
    sent += fan_out("ep", n_ep, me, lambda t: slot_send.at[t], slot_land, slot_ss, slot_rs)
    slot_land[me] = slot_send[me]
    lanes = dense_mix.shape[1]
    mix_sum = jnp.zeros((rows, lanes), F32)
    for index in range(model // lanes):
        mix_sum = mix_sum + ffn_in[:, index * lanes : (index + 1) * lanes].astype(F32) * dense_mix[
            index : index + 1, :
        ].astype(F32)
    mix = jax.nn.sigmoid(jnp.sum(mix_sum, axis=-1, keepdims=True))

    chip_collect("ep", half, me, dense_land, dense_ss, dense_rs)
    dense_sum = total_of(dense_land, half) * row_scale
    dense_first = dense_sum[:, :hidden]
    hidden_send[...] = (
        dense_first / (1.0 + jnp.exp(-dense_first)) * dense_sum[:, hidden:]
    ).astype(BF16)
    sent += fan_out("ep", n_ep, me, lambda t: hidden_send, hidden_land, hidden_ss, hidden_rs)
    hidden_land[me] = hidden_send[...]

    collect("ep", n_ep, me, slot_land, slot_ss, slot_rs)
    for load in loads[8:]:
        load.wait()
    slot_rows = jnp.concatenate(
        [slot_land[index].astype(F32) for index in range(n_ep)], axis=0
    ).astype(BF16)
    gate_part = dot32(slot_rows, expert_gate_held[0])
    up_part = dot32(slot_rows, expert_up_held[0])
    expert_hidden = (gate_part / (1.0 + jnp.exp(-gate_part)) * up_part).astype(BF16)
    chunk = model // n_tp
    for index in range(n_tp):
        expert_send[index] = dot32(
            expert_hidden, expert_down_held[0, :, index * chunk : (index + 1) * chunk]
        ).astype(BF16)
    sent += fan_out(
        "tp", n_tp, me_tp, lambda t: expert_send.at[t], expert_land, expert_ss, expert_rs
    )
    expert_land[me_tp] = expert_send[me_tp]

    collect("tp", n_tp, me_tp, expert_land, expert_ss, expert_rs)
    expert_total = total_of(expert_land, n_tp)
    for index in range(n_ep):
        back_send[index] = expert_total[index * slots : (index + 1) * slots].astype(BF16)
    sent += fan_out("ep", n_ep, me, lambda t: back_send.at[t], back_land, back_ss, back_rs)
    back_land[me] = back_send[me]

    collect("ep", n_ep, me, hidden_land, hidden_ss, hidden_rs)
    down = dot32(hidden_land[...].reshape(n_ep * rows, hidden), dense_down_held[...])
    down_send[...] = down.astype(BF16).reshape(n_tp, group_rows, depth)
    sent += fan_out("tp", n_tp, me_tp, lambda t: down_send.at[t], down_land, down_ss, down_rs)
    down_land[me_tp] = down_send[me_tp]

    collect("ep", n_ep, me, back_land, back_ss, back_rs)
    back_rows = jnp.concatenate(
        [back_land[index].astype(F32) for index in range(n_ep)], axis=0
    ).astype(BF16)
    route_send[...] = first_route * pick(to_first, back_rows) + second_route * pick(
        to_second, back_rows
    )
    sent += fan_out("tp", n_tp, me_tp, lambda t: route_send, route_land, route_ss, route_rs)
    route_land[me_tp] = route_send[...]

    collect("tp", n_tp, me_tp, down_land, down_ss, down_rs)
    tail_send[...] = total_of(down_land, n_tp).astype(BF16).reshape(ratio, rows, depth)
    spread_rows("ep", "tp", *grid, tail_send, tail_land, tail_ss, tail_rs)
    collect("tp", n_tp, me_tp, route_land, route_ss, route_rs)
    spread_wait("ep", "tp", *grid, tail_send, tail_land, tail_ss, tail_rs)
    for index in range(n_ep):
        full[:, index * depth : (index + 1) * depth] = tail_land[index].astype(F32)
    for index in range(n_tp):
        span = slice(index * chunk, (index + 1) * chunk)
        out[:, span] = (
            residual[:, span].astype(F32) + route_land[index] + mix * full[:, span]
        ).astype(BF16)
    for copy in sent:
        copy.wait_send()
    spread_sent("ep", "tp", *grid, mix_send, mix_land, mix_ss, mix_rs)
    spread_sent("ep", "tp", *grid, tail_send, tail_land, tail_ss, tail_rs)


def layer(n_ep, n_tp, slots, scalars, small, large):
    rows, model = small[0].shape
    depth, hidden = large[0].shape
    heads, span, size = large[3].shape[1:]
    group_rows = n_ep * rows // n_tp
    ratio = n_ep // n_tp
    half = n_ep // 2
    chunk = model // n_tp
    vmem = pl.BlockSpec(memory_space=pltpu.VMEM)
    smem = pl.BlockSpec(memory_space=pltpu.SMEM)
    hbm = pl.BlockSpec(memory_space=pltpu.HBM)
    return pl.pallas_call(
        functools.partial(layer_kernel, n_ep, n_tp),
        out_shape=jax.ShapeDtypeStruct((rows, model), BF16),
        in_specs=[smem] * 2 + [vmem] * len(small) + [hbm] * len(large),
        out_specs=vmem,
        scratch_shapes=[
            pltpu.VMEM(large[0].shape, BF16),
            pltpu.VMEM(large[1].shape, BF16),
            pltpu.VMEM(large[2].shape, BF16),
            pltpu.VMEM(large[3].shape, BF16),
            pltpu.VMEM(large[4].shape, BF16),
            pltpu.VMEM(large[5].shape, BF16),
            pltpu.VMEM(large[6].shape, BF16),
            pltpu.VMEM(large[7].shape, BF16),
            pltpu.VMEM(large[8].shape, BF16),
            pltpu.VMEM(large[9].shape, BF16),
            pltpu.VMEM(large[10].shape, BF16),
            pltpu.VMEM(large[11].shape, BF16),
            pltpu.SemaphoreType.DMA((12,)),
            pltpu.VMEM((n_ep, rows, depth), BF16),
            pltpu.VMEM((n_ep, rows, depth), BF16),
            pltpu.SemaphoreType.DMA((n_ep,)),
            pltpu.SemaphoreType.DMA((n_ep,)),
            pltpu.VMEM((3, 2, half, rows, hidden), F32),
            pltpu.VMEM((3, half, rows, hidden), F32),
            pltpu.SemaphoreType.DMA((3,)),
            pltpu.SemaphoreType.DMA((3,)),
            pltpu.VMEM((2, half, rows, hidden), F32),
            pltpu.VMEM((2, half, rows, hidden), F32),
            pltpu.SemaphoreType.DMA((2, half)),
            pltpu.SemaphoreType.DMA((2, half)),
            pltpu.VMEM((half, rows, hidden), BF16),
            pltpu.VMEM((half, rows, hidden), BF16),
            pltpu.SemaphoreType.DMA((half,)),
            pltpu.SemaphoreType.DMA((half,)),
            pltpu.VMEM((rows, heads, size), F32),
            pltpu.VMEM((rows, heads, size), F32),
            pltpu.VMEM((rows, heads, size), F32),
            pltpu.VMEM((rows, heads, size), F32),
            pltpu.VMEM((rows, heads, span), F32),
            pltpu.VMEM((rows, heads, size), F32),
            pltpu.VMEM((rows, hidden), BF16),
            pltpu.VMEM((rows, model), F32),
            pltpu.VMEM((n_ep, rows, hidden), BF16),
            pltpu.SemaphoreType.DMA((n_ep,)),
            pltpu.SemaphoreType.DMA((n_ep,)),
            pltpu.VMEM((n_tp, group_rows, depth), F32),
            pltpu.VMEM((n_tp, group_rows, depth), F32),
            pltpu.SemaphoreType.DMA((n_tp,)),
            pltpu.SemaphoreType.DMA((n_tp,)),
            pltpu.VMEM((ratio, rows, depth), F32),
            pltpu.VMEM((n_ep, rows, depth), F32),
            pltpu.SemaphoreType.DMA((n_ep,)),
            pltpu.SemaphoreType.DMA((n_ep,)),
            pltpu.VMEM((n_ep, rows, depth), BF16),
            pltpu.VMEM((n_ep, rows, depth), BF16),
            pltpu.SemaphoreType.DMA((n_ep,)),
            pltpu.SemaphoreType.DMA((n_ep,)),
            pltpu.VMEM((n_tp, ratio, rows, depth), F32),
            pltpu.SemaphoreType.DMA((n_tp,)),
            pltpu.SemaphoreType.DMA((n_tp,)),
            pltpu.VMEM((n_ep, slots, model), BF16),
            pltpu.VMEM((n_ep, slots, model), BF16),
            pltpu.SemaphoreType.DMA((n_ep,)),
            pltpu.SemaphoreType.DMA((n_ep,)),
            pltpu.VMEM((2, half, rows, 2 * hidden), F32),
            pltpu.VMEM((half, rows, 2 * hidden), F32),
            pltpu.SemaphoreType.DMA((1,)),
            pltpu.SemaphoreType.DMA((1,)),
            pltpu.VMEM((half, rows, 2 * hidden), BF16),
            pltpu.VMEM((half, rows, 2 * hidden), BF16),
            pltpu.SemaphoreType.DMA((half,)),
            pltpu.SemaphoreType.DMA((half,)),
            pltpu.VMEM((n_tp, n_ep * slots, chunk), BF16),
            pltpu.VMEM((n_tp, n_ep * slots, chunk), BF16),
            pltpu.SemaphoreType.DMA((n_tp,)),
            pltpu.SemaphoreType.DMA((n_tp,)),
            pltpu.VMEM((n_ep, slots, chunk), BF16),
            pltpu.VMEM((n_ep, slots, chunk), BF16),
            pltpu.SemaphoreType.DMA((n_ep,)),
            pltpu.SemaphoreType.DMA((n_ep,)),
            pltpu.VMEM((rows, hidden), BF16),
            pltpu.VMEM((n_ep, rows, hidden), BF16),
            pltpu.SemaphoreType.DMA((n_ep,)),
            pltpu.SemaphoreType.DMA((n_ep,)),
            pltpu.VMEM((n_tp, group_rows, depth), BF16),
            pltpu.VMEM((n_tp, group_rows, depth), BF16),
            pltpu.SemaphoreType.DMA((n_tp,)),
            pltpu.SemaphoreType.DMA((n_tp,)),
            pltpu.VMEM((ratio, rows, depth), BF16),
            pltpu.VMEM((n_ep, rows, depth), BF16),
            pltpu.SemaphoreType.DMA((n_ep,)),
            pltpu.SemaphoreType.DMA((n_ep,)),
            pltpu.VMEM((rows, chunk), F32),
            pltpu.VMEM((n_tp, rows, chunk), F32),
            pltpu.SemaphoreType.DMA((n_tp,)),
            pltpu.SemaphoreType.DMA((n_tp,)),
        ],
        compiler_params=pltpu.CompilerParams(
            collective_id=0, has_side_effects=True, vmem_limit_bytes=60 * 1024 * 1024
        ),
    )(*scalars, *small, *large)


def shards(
    tokens,
    attn_gain,
    query_weight,
    key_weight,
    value_weight,
    forget_weight,
    forget_bias,
    cache_keys,
    cache_values,
    cache_gates,
    lengths,
    output_weight,
    ffn_gain,
    dense_gate_proj,
    dense_up_proj,
    dense_down_proj,
    dense_mix,
    expert_ids,
    group_prob,
    pair_prob,
    expert_gate,
    expert_up,
    expert_down,
):
    seq_count = tokens.shape[0]
    n_ep = lax.axis_size("ep")
    n_tp = lax.axis_size("tp")
    expert_count = n_ep * expert_gate.shape[0]
    capacity = max(4 * seq_count // expert_count, 8)
    model = (1, tokens.shape[1])
    return layer(
        n_ep,
        n_tp,
        capacity,
        (forget_bias.reshape(1, -1), lengths.reshape(1, -1)),
        (
            tokens,
            attn_gain.reshape(model),
            forget_weight.T,
            cache_gates,
            ffn_gain.reshape(model),
            ffn_gain.reshape(n_ep, 1, -1),
            dense_mix.reshape(-1, 128),
            expert_ids.T,
            group_prob.reshape(1, -1),
            pair_prob.T,
        ),
        (
            query_weight,
            key_weight,
            value_weight,
            cache_keys,
            cache_values,
            output_weight,
            dense_gate_proj,
            dense_up_proj,
            expert_gate,
            expert_up,
            expert_down,
            dense_down_proj,
        ),
    )


def solution(mesh):
    return jax.shard_map(
        shards,
        mesh=mesh,
        in_specs=(
            P("ep", None),
            P(),
            P("ep", "tp"),
            P("ep", "tp"),
            P("ep", "tp"),
            P(None, "tp"),
            P("tp"),
            P("ep", "tp", None, None),
            P("ep", "tp", None, None),
            P("ep", "tp", None),
            P("ep"),
            P("tp", "ep"),
            P(),
            P("ep", "tp"),
            P("ep", "tp"),
            P("tp", "ep"),
            P(),
            P("ep", None),
            P("ep"),
            P("ep", None),
            P("ep", None, "tp"),
            P("ep", None, "tp"),
            P("ep", "tp", None),
        ),
        out_specs=P("ep", None),
        check_vma=False,
    )
```

```python
import functools
import math

import jax
import jax.numpy as jnp
from jax import lax
from jax.experimental import pallas as pl
from jax.experimental.pallas import tpu as pltpu
from jax.sharding import PartitionSpec as P

EPSILON = 1e-06


def rms_scale(values, norm_gain):
    widened = values.astype(jnp.float32)
    return (
        widened
        * lax.rsqrt(jnp.mean(widened * widened, axis=-1, keepdims=True) + EPSILON)
        * norm_gain
    )


MESH = pl.DeviceIdType.MESH
F32 = jnp.float32
BF16 = jnp.bfloat16


def flip(me, step):
    bit = 1
    while bit <= step:
        if step & bit:
            me = me + bit - 2 * bit * lax.rem(me // bit, 2)
        bit *= 2
    return me


def toward(me, step, count):
    return flip(me, step) if count & (count - 1) == 0 else lax.rem(me + step, count)


def origin(me, step, count):
    return flip(me, step) if count & (count - 1) == 0 else lax.rem(me + count - step, count)


def far_first(count):
    return range(count - 1, 0, -1)


def remote(source, place, send_sem, recv_sem, device):
    return pltpu.make_async_remote_copy(
        src_ref=source,
        dst_ref=place,
        send_sem=send_sem,
        recv_sem=recv_sem,
        device_id=device,
        device_id_type=MESH,
    )


def fan_out(axis, count, me, source_of, landing, send_sem, recv_sem, slot=None):
    copies = []
    place = me if slot is None else slot(me)
    for step in far_first(count):
        target = toward(me, step, count)
        copy = remote(
            source_of(target),
            landing.at[place],
            send_sem.at[step],
            recv_sem.at[me],
            {axis: target},
        )
        copy.start()
        copies.append(copy)
    return copies


def arrive(axis, source, place, send_sem, recv_sem):
    remote(place, place, send_sem, recv_sem, {axis: source}).wait_recv()


def collect(axis, count, me, landing, send_sem, recv_sem, slot=None):
    for step in range(1, count):
        source = origin(me, step, count)
        place = source if slot is None else slot(source)
        arrive(axis, source, landing.at[place], send_sem.at[step], recv_sem.at[source])


def total_of(ref, count):
    total = ref[0].astype(F32)
    for index in range(1, count):
        total = total + ref[index].astype(F32)
    return total


def dot32(left, right):
    return jnp.dot(left, right, preferred_element_type=F32)


def silu(values):
    return values / (1.0 + jnp.exp(-values))


def chip_order(index, half):
    return lax.rem(index, 2) * half + index // 2


def pair_copy(axis, me, source, landing, send_sem, recv_sem, slot):
    return remote(
        source,
        landing,
        send_sem.at[slot],
        recv_sem.at[slot],
        {axis: me + 1 - 2 * lax.rem(me, 2)},
    )


def chip_fan(axis, half, me, held, landing, send_sem, recv_sem):
    chip, core = me // 2, lax.rem(me, 2)
    copies = []
    for step in far_first(half):
        target = toward(chip, step, half)
        copy = remote(
            held.at[target],
            landing.at[chip],
            send_sem.at[step],
            recv_sem.at[chip],
            {axis: target * 2 + core},
        )
        copy.start()
        copies.append(copy)
    landing[chip] = held[chip]
    return copies


def chip_collect(axis, half, me, landing, send_sem, recv_sem):
    chip, core = me // 2, lax.rem(me, 2)
    for step in range(1, half):
        source = origin(chip, step, half)
        arrive(
            axis, source * 2 + core, landing.at[source], send_sem.at[step], recv_sem.at[source]
        )


def pick(one_hot, held):
    return lax.dot_general(
        one_hot, held, (((0,), (0,)), ((), ())), preferred_element_type=F32
    )


def slot_tables(ids, experts, slots):
    rows = ids.shape[1]
    row_at = lax.broadcasted_iota(jnp.int32, (rows, rows), 0)
    row_to = lax.broadcasted_iota(jnp.int32, (rows, rows), 1)
    expert_at = lax.broadcasted_iota(jnp.int32, (experts, rows), 0).astype(F32)
    slot_at = lax.broadcasted_iota(jnp.int32, (slots, rows), 0).astype(F32)
    first = ids[0:1, :] == expert_at
    second = ids[1:2, :] == expert_at
    hits = (first | second).astype(F32).astype(BF16)
    earlier = (row_at < row_to).astype(F32).astype(BF16)
    ranks = dot32(hits, earlier)
    tables = []
    for chosen in (first, second):
        place = jnp.where(chosen, ranks, -1.0)
        tables.append(
            jnp.concatenate(
                [
                    (place[expert : expert + 1, :] == slot_at).astype(F32)
                    for expert in range(experts)
                ],
                axis=0,
            )
        )
    return tables


def route_columns(group_prob, pair_prob):
    rows = pair_prob.shape[1]
    row_at = lax.broadcasted_iota(jnp.int32, (rows, rows), 0)
    row_to = lax.broadcasted_iota(jnp.int32, (rows, rows), 1)
    probs = pair_prob[...]
    shares = group_prob[...] * probs / (probs[0:1, :] + probs[1:2, :])
    return [
        jnp.sum(jnp.where(row_at == row_to, shares[k : k + 1, :], 0.0), axis=-1, keepdims=True)
        for k in range(2)
    ]


def layer_kernel(
    n_ep,
    n_tp,
    forget_bias,
    lengths,
    tokens,
    attn_gain,
    forget_rows,
    gates,
    gain,
    gain_parts,
    dense_mix,
    expert_ids,
    group_prob,
    pair_prob,
    query_weight,
    key_weight,
    value_weight,
    keys,
    values,
    output_weight,
    dense_gate,
    dense_up,
    expert_gate,
    expert_up,
    expert_down,
    dense_down,
    out,
    query_weight_held,
    key_weight_held,
    value_weight_held,
    keys_held,
    values_held,
    output_weight_held,
    dense_gate_held,
    dense_up_held,
    expert_gate_held,
    expert_up_held,
    expert_down_held,
    dense_down_held,
    load_sem,
    norm_send,
    norm_land,
    norm_ss,
    norm_rs,
    ids_send,
    ids_land,
    ids_ss,
    ids_rs,
    token_send,
    token_land,
    token_ss,
    token_rs,
    part_send,
    part_land,
    part_ss,
    part_rs,
    score_send,
    score_land,
    score_ss,
    score_rs,
    value_send,
    value_land,
    value_ss,
    value_rs,
    query_rows,
    key_rows,
    value_rows,
    forget_logs,
    scores,
    mixed,
    attended,
    att_land,
    att_ss,
    att_rs,
    head_send,
    head_land,
    head_ss,
    head_rs,
    res_land,
    res_send,
    res_ss,
    res_rs,
    own_land,
    own_ss,
    own_rs,
    slot_send,
    slot_land,
    slot_ss,
    slot_rs,
    pass_ss,
    pass_rs,
    ffn_rows,
    mix_parts,
    pair_send,
    pair_land,
    pair_ss,
    pair_rs,
    dense_send,
    dense_land,
    dense_ss,
    dense_rs,
    hidden_send,
    hidden_land,
    hidden_ss,
    hidden_rs,
    expert_send,
    expert_land,
    expert_ss,
    expert_rs,
    back_send,
    back_land,
    back_ss,
    back_rs,
    tail_send,
    tail_land,
    tail_ss,
    tail_rs,
    quarter_land,
    quarter_ss,
    quarter_rs,
    route_part,
    out_send,
    out_land,
    out_ss,
    out_rs,
):
    me = lax.axis_index("ep")
    me_tp = lax.axis_index("tp")
    barrier = pltpu.get_barrier_semaphore()
    ratio = n_ep // n_tp
    half = n_ep // 2
    chip, core = me // 2, lax.rem(me, 2)
    spreads = me // ratio == me_tp
    part_at = lax.rem(me, ratio)

    def greet(axis, mine, count):
        def signal(step, carry):
            pl.semaphore_signal(
                barrier,
                inc=1,
                device_id={axis: lax.rem(mine + step, count)},
                device_id_type=MESH,
            )
            return carry

        lax.fori_loop(1, count, signal, 0, unroll=count <= 8)

    greet("ep", me, n_ep)
    greet("tp", me_tp, n_tp)
    sources = [query_weight, key_weight, value_weight, keys, values, output_weight, dense_gate, dense_up, expert_gate, expert_up, dense_down]
    places = [query_weight_held, key_weight_held, value_weight_held, keys_held, values_held, output_weight_held, dense_gate_held, dense_up_held, expert_gate_held, expert_up_held, dense_down_held]
    rows, model = tokens.shape
    depth, hidden = query_weight.shape
    heads, span, size = keys.shape[1:]
    slots = slot_send.shape[2]
    chunk = model // n_tp
    wide = 2 * hidden
    for index in range(n_tp):
        sources.append(expert_down.at[0, :, pl.ds(index * chunk, chunk)])
        places.append(expert_down_held.at[index])
    loads = [
        pltpu.make_async_copy(source, place, load_sem.at[index])
        for index, (source, place) in enumerate(zip(sources, places))
    ]
    for load in loads:
        load.start()

    def order(index):
        return chip_order(index, half)

    normed = rms_scale(tokens[...], attn_gain[...])
    for index in range(n_ep):
        norm_send[index] = normed[:, index * depth : (index + 1) * depth].astype(BF16)
        token_send[index] = tokens[:, index * depth : (index + 1) * depth]
    ids = expert_ids[...].astype(F32)
    ids_send[0:2, 0:rows] = ids
    pl.semaphore_wait(barrier, n_ep + n_tp - 2)

    sent = fan_out("ep", n_ep, me, lambda t: norm_send.at[t], norm_land, norm_ss, norm_rs, order)
    norm_land[order(me)] = norm_send[me]

    def row_copies(source_of, landing, send_sem, recv_sem):
        return [
            remote(
                source_of(toward(me, step, n_ep)),
                landing.at[part_at],
                send_sem.at[step],
                recv_sem.at[part_at],
                {"ep": toward(me, step, n_ep)},
            )
            for step in far_first(n_ep)
        ]

    def row_arrivals(base, landing, send_sem, recv_sem):
        for part in range(ratio):
            source = base * ratio + part

            @pl.when(source != me)
            def _():
                arrive("ep", source, landing.at[part], send_sem.at[0], recv_sem.at[part])

    spread_early = row_copies(lambda t: token_send.at[t], token_land, token_ss, token_rs)
    spread_early += row_copies(lambda t: ids_send, ids_land, ids_ss, ids_rs)

    @pl.when(spreads)
    def _():
        for copy in spread_early:
            copy.start()
        token_land[part_at] = token_send[me]
        ids_land[part_at] = ids_send[...]

    normed_wide = normed.astype(BF16).astype(F32)
    for head in range(heads):
        logit = forget_bias[0, head] + jnp.sum(
            normed_wide * forget_rows[head : head + 1, :].astype(F32), axis=-1, keepdims=True
        )
        forget_log = jnp.minimum(logit, 0.0) - jnp.log1p(jnp.exp(-jnp.abs(logit)))
        forget_logs[:, head, :] = jnp.broadcast_to(forget_log, (rows, size))
    mix_lanes = dense_mix.shape[1]
    mix_wide = dense_mix[...].astype(F32)
    for index in range(n_ep):
        for start in range(0, depth, min(depth, mix_lanes)):
            at = index * depth + start
            line, lane = at // mix_lanes, at % mix_lanes
            width = min(depth, mix_lanes)
            mix_parts[index, :, start : start + width] = mix_wide[
                line : line + 1, lane : lane + width
            ]
    first_table, second_table = slot_tables(ids, n_ep, slots)
    to_first, to_second = first_table.astype(BF16), second_table.astype(BF16)
    first_route, second_route = route_columns(group_prob, pair_prob)

    collect("ep", n_ep, me, norm_land, norm_ss, norm_rs, order)
    joined = norm_land[...].reshape(n_ep * rows, depth)
    swaps = []
    for index, weight in enumerate((query_weight_held, key_weight_held, value_weight_held)):
        loads[index].wait()
        part_send[index] = dot32(joined, weight[...]).reshape(2, half, rows, hidden)
        swap = pair_copy(
            "ep", me, part_send.at[index, 1 - core], part_land.at[index], part_ss, part_rs, index
        )
        swap.start()
        swaps.append(swap)
    sent += swaps
    for index in range(2):
        swaps[index].wait_recv()
        score_send[index] = part_send[index, core] + part_land[index]
        sent += chip_fan(
            "ep",
            half,
            me,
            score_send.at[index],
            score_land.at[index],
            score_ss.at[index],
            score_rs.at[index],
        )
    swaps[2].wait_recv()
    value_send[...] = (part_send[2, core] + part_land[2]).astype(BF16)
    sent += chip_fan("ep", half, me, value_send, value_land, value_ss, value_rs)
    row_arrivals(me_tp, ids_land, ids_ss, ids_rs)
    dispatch = []
    for part in range(ratio):
        tables = slot_tables(ids_land[part][0:2, 0:rows], n_ep, slots)
        dispatch.append((tables[0] + tables[1]).astype(BF16))
    row_arrivals(me_tp, token_land, token_ss, token_rs)
    chip_collect("ep", half, me, score_land.at[0], score_ss.at[0], score_rs.at[0])
    summed = total_of(score_land.at[0], half).astype(BF16).astype(F32)
    for head in range(heads):
        query_rows[:, head, :] = summed[:, head * size : (head + 1) * size]

    scale = 1.0 / math.sqrt(size)
    loads[3].wait()
    loads[4].wait()

    def score_step(seq, carry):
        for head in range(heads):
            query = query_rows[seq, head : head + 1, :].astype(BF16)
            scores[seq, head : head + 1, :] = lax.dot_general(
                query,
                keys_held[seq, head],
                (((1,), (1,)), ((), ())),
                preferred_element_type=F32,
            )
        return carry

    lax.fori_loop(0, rows, score_step, 0, unroll=4)
    chip_collect("ep", half, me, score_land.at[1], score_ss.at[1], score_rs.at[1])
    summed = total_of(score_land.at[1], half).astype(BF16).astype(F32)
    for head in range(heads):
        key_rows[:, head, :] = summed[:, head * size : (head + 1) * size]
    positions = lax.broadcasted_iota(jnp.int32, (rows, heads, span), 2)
    sequences = lax.broadcasted_iota(jnp.int32, (rows, heads, size), 0)
    live_wide = jnp.zeros((rows, heads, size), jnp.int32)
    for seq in range(rows):
        live_wide = jnp.where(sequences == seq, lengths[0, seq], live_wide)
    lives = live_wide[:, :, 0:1]
    gate_all = gates[...]
    last_gate = jnp.sum(jnp.where(positions == lives - 1, gate_all, 0.0), axis=-1, keepdims=True)
    gate_now = last_gate + forget_logs[:, :, 0:1]
    score_all = scores[...] * scale + gate_now - gate_all
    score_all = jnp.where(positions < lives, score_all, -jnp.inf)
    own_score = jnp.sum(query_rows[...] * key_rows[...], axis=-1, keepdims=True) * scale
    row_top = jnp.maximum(jnp.max(score_all, axis=-1, keepdims=True), own_score)
    raised = jnp.exp(score_all - row_top)
    own_raised = jnp.exp(own_score - row_top)
    totals = jnp.sum(raised, axis=-1, keepdims=True) + own_raised
    scores[...] = raised / totals
    own_prob = (own_raised / totals).astype(BF16).astype(F32)

    def value_step(seq, carry):
        for head in range(heads):
            weight = scores[seq, head : head + 1, :].astype(BF16)
            mixed[seq, head : head + 1, :] = dot32(weight, values_held[seq, head])
        return carry

    lax.fori_loop(0, rows, value_step, 0, unroll=4)
    chip_collect("ep", half, me, value_land, value_ss, value_rs)
    value_sum = total_of(value_land, half).astype(BF16).astype(F32)
    for head in range(heads):
        value_rows[:, head, :] = value_sum[:, head * size : (head + 1) * size]
    mixed[...] = mixed[...] + own_prob * value_rows[...]
    for head in range(heads):
        attended[:, head * size : (head + 1) * size] = mixed[:, head, :].astype(BF16)

    sent += fan_out("ep", n_ep, me, lambda t: attended, att_land, att_ss, att_rs)
    att_land[me] = attended[...]
    collect("ep", n_ep, me, att_land, att_ss, att_rs)
    loads[5].wait()
    shares = dot32(att_land[...].reshape(n_ep * rows, hidden), output_weight_held[...])
    head_send[...] = shares.reshape(n_tp, ratio, rows, depth)
    sent += fan_out("tp", n_tp, me_tp, lambda t: head_send.at[t], head_land, head_ss, head_rs)
    head_land[me_tp] = head_send[me_tp]
    collect("tp", n_tp, me_tp, head_land, head_ss, head_rs)
    residual = (token_land[...].astype(F32) + total_of(head_land, n_tp)).astype(BF16)
    res_send[...] = residual
    sent += fan_out("tp", n_tp, me_tp, lambda t: res_send, res_land, res_ss, res_rs)
    for part in range(ratio):
        picked = dot32(dispatch[part], residual[part])
        slot_send[:, part] = picked.reshape(n_ep, slots, depth).astype(BF16)
    sent += fan_out(
        "ep", n_ep, me, lambda t: slot_send.at[t], slot_land.at[me_tp], slot_ss, slot_rs
    )
    slot_land[me_tp, me] = slot_send[me]
    res_land[me_tp] = residual

    def forward(source):
        for step in far_first(n_tp):
            remote(
                slot_land.at[me_tp, source],
                slot_land.at[me_tp, source],
                pass_ss.at[step],
                pass_rs.at[me_tp],
                {"tp": toward(me_tp, step, n_tp)},
            ).start()

    def relay(step):
        source = origin(me, step, n_ep)
        arrive("ep", source, slot_land.at[me_tp, source], slot_ss.at[step], slot_rs.at[source])
        forward(source)

    forward(me)
    early = min(4, n_ep)
    for step in range(1, early):
        relay(step)

    collect("tp", n_tp, me_tp, res_land, res_ss, res_rs)
    held = res_land[...].reshape(n_ep * rows, depth).astype(F32)
    dense_rows = (held * gain_parts[me]).astype(BF16)
    squares = jnp.sum(held * held, axis=-1, keepdims=True)
    mixes = jnp.sum(dense_rows.astype(F32) * mix_parts[me], axis=-1, keepdims=True)
    lane_at = lax.broadcasted_iota(jnp.int32, (n_ep * rows, 128), 1)
    sums = jnp.where(lax.rem(lane_at, 2) == 0, squares, mixes)
    loads[6].wait()
    loads[7].wait()
    products = (
        (0, hidden, dot32(dense_rows, dense_gate_held[...])),
        (hidden, wide, dot32(dense_rows, dense_up_held[...])),
        (wide, wide + 128, sums),
    )
    for start, stop, product in products:
        for place in range(n_ep):
            pair_send[place % 2, place // 2, :, start:stop] = product[
                place * rows : (place + 1) * rows
            ]
    swap = pair_copy("ep", me, pair_send.at[1 - core], pair_land, pair_ss, pair_rs, 0)
    swap.start()
    sent.append(swap)
    owner_copies = row_copies(
        lambda t: res_land.at[t // ratio, lax.rem(t, ratio)], own_land, own_ss, own_rs
    )
    for step in range(early, n_ep):
        relay(step)
    swap.wait_recv()
    paired = pair_send[core] + pair_land[...]
    dense_send[:, :, :wide] = paired[:, :, :wide].astype(BF16)
    tail = paired[:, :, wide:]
    coarse = tail.astype(BF16)
    fine = (tail - coarse.astype(F32)).astype(BF16)
    lane_at = lax.broadcasted_iota(jnp.int32, (half, rows, 128), 2)
    dense_send[:, :, wide:] = jnp.where(
        lane_at < 2, coarse.astype(F32), fine.astype(F32)
    ).astype(BF16)
    sent += chip_fan("ep", half, me, dense_send, dense_land, dense_ss, dense_rs)

    @pl.when(spreads)
    def _():
        for copy in owner_copies:
            copy.start()
        own_land[part_at] = res_land[me // ratio, part_at]

    for step in range(1, n_tp):
        source = origin(me_tp, step, n_tp)
        arrive("tp", source, slot_land.at[source], pass_ss.at[step], pass_rs.at[source])
    total_slots = n_tp * ratio * slots
    square = jnp.zeros((total_slots, depth), F32)
    for index in range(n_ep):
        part = slot_land[:, index].astype(F32).reshape(total_slots, depth)
        square = square + part * part
    slot_scale = lax.rsqrt(jnp.sum(square, axis=-1, keepdims=True) / model + EPSILON)
    for index in range(n_ep):
        part = slot_land[:, index].astype(F32).reshape(total_slots, depth)
        ffn_rows[:, index * depth : (index + 1) * depth] = (
            part * slot_scale * gain_parts[index]
        ).astype(BF16)
    for load in loads[8:]:
        load.wait()
    ffn_in = ffn_rows[...]
    expert_hidden = (
        silu(dot32(ffn_in, expert_gate_held[0])) * dot32(ffn_in, expert_up_held[0])
    ).astype(BF16)
    for step in far_first(n_tp):
        target = toward(me_tp, step, n_tp)
        expert_send[target] = dot32(expert_hidden, expert_down_held[target]).astype(BF16)
        copy = remote(
            expert_send.at[target],
            expert_land.at[me_tp],
            expert_ss.at[step],
            expert_rs.at[me_tp],
            {"tp": target},
        )
        copy.start()
        sent.append(copy)
    expert_land[me_tp] = dot32(expert_hidden, expert_down_held[me_tp]).astype(BF16)

    chip_collect("ep", half, me, dense_land, dense_ss, dense_rs)
    dense_sum = total_of(dense_land, half)
    sums = dense_sum[:, wide:]
    row_scale = lax.rsqrt((sums[:, 0:1] + sums[:, 2:3]) / model + EPSILON)
    mix = jax.nn.sigmoid((sums[:, 1:2] + sums[:, 3:4]) * row_scale)
    dense_pair = dense_sum[:, :wide] * row_scale
    hidden_send[...] = (silu(dense_pair[:, :hidden]) * dense_pair[:, hidden:]).astype(BF16)
    sent += fan_out("ep", n_ep, me, lambda t: hidden_send, hidden_land, hidden_ss, hidden_rs)
    hidden_land[me] = hidden_send[...]

    collect("ep", n_ep, me, hidden_land, hidden_ss, hidden_rs)
    down = dot32(hidden_land[...].reshape(n_ep * rows, hidden), dense_down_held[...])
    tail_send[...] = down.astype(BF16).reshape(n_ep, rows, depth)
    sent += fan_out("ep", n_ep, me, lambda t: tail_send.at[t], tail_land, tail_ss, tail_rs)
    tail_land[me] = tail_send[me]

    collect("tp", n_tp, me_tp, expert_land, expert_ss, expert_rs)
    expert_total = total_of(expert_land, n_tp)
    for index in range(n_ep):
        back_send[index] = expert_total[index * slots : (index + 1) * slots].astype(BF16)
    sent += fan_out("ep", n_ep, me, lambda t: back_send.at[t], back_land, back_ss, back_rs)
    back_land[me] = back_send[me]

    def quarter_copy(source):
        return remote(
            tail_land.at[source],
            quarter_land.at[me_tp, lax.rem(source, ratio)],
            quarter_ss.at[source],
            quarter_rs.at[me_tp, lax.rem(source, ratio)],
            {"tp": source // ratio},
        )

    for step in range(n_ep):
        source = me if step == 0 else origin(me, step, n_ep)
        if step:
            arrive("ep", source, tail_land.at[source], tail_ss.at[step], tail_rs.at[source])

        @pl.when(source // ratio != me_tp)
        def _():
            quarter_copy(source).start()

        @pl.when(source // ratio == me_tp)
        def _():
            quarter_land[me_tp, lax.rem(source, ratio)] = tail_land[source]

    collect("ep", n_ep, me, back_land, back_ss, back_rs)
    back_rows = jnp.concatenate(
        [back_land[index].astype(F32) for index in range(n_ep)], axis=0
    ).astype(BF16)
    route_part[...] = first_route * pick(to_first, back_rows) + second_route * pick(
        to_second, back_rows
    )
    row_arrivals(me_tp, own_land, own_ss, own_rs)
    for step in range(1, n_tp):
        source = origin(me_tp, step, n_tp)
        for part in range(ratio):
            arrive(
                "tp",
                source,
                quarter_land.at[source, part],
                quarter_ss.at[0],
                quarter_rs.at[source, part],
            )
    for part in range(ratio):
        columns = slice(part * depth, (part + 1) * depth)
        out_send[:, columns] = (
            own_land[part].astype(F32)
            + route_part[:, columns]
            + mix * total_of(quarter_land.at[:, part], n_tp)
        ).astype(BF16)
    sent += fan_out("tp", n_tp, me_tp, lambda t: out_send, out_land, out_ss, out_rs)
    out_land[me_tp] = out_send[...]
    for copy in sent[:-1]:
        copy.wait_send()
    for step in range(1, n_tp):
        remote(
            slot_land.at[me_tp],
            slot_land.at[me_tp],
            pass_ss.at[step],
            pass_rs.at[me_tp],
            {"tp": toward(me_tp, step, n_tp)},
        ).wait_send()

    @pl.when(spreads)
    def _():
        for copy in spread_early + owner_copies:
            copy.wait_send()

    for source in range(n_ep):

        @pl.when(source // ratio != me_tp)
        def _():
            quarter_copy(source).wait_send()

    collect("tp", n_tp, me_tp, out_land, out_ss, out_rs)
    for index in range(n_tp):
        out[:, index * chunk : (index + 1) * chunk] = out_land[index]
    sent[-1].wait_send()


def layer(n_ep, n_tp, slots, scalars, small, large):
    rows, model = small[0].shape
    depth, hidden = large[0].shape
    heads, span, size = large[3].shape[1:]
    ratio = n_ep // n_tp
    half = n_ep // 2
    chunk = model // n_tp
    vmem = pl.BlockSpec(memory_space=pltpu.VMEM)
    smem = pl.BlockSpec(memory_space=pltpu.SMEM)
    hbm = pl.BlockSpec(memory_space=pltpu.HBM)
    return pl.pallas_call(
        functools.partial(layer_kernel, n_ep, n_tp),
        out_shape=jax.ShapeDtypeStruct((rows, model), BF16),
        in_specs=[smem] * 2 + [vmem] * len(small) + [hbm] * len(large),
        out_specs=vmem,
        scratch_shapes=[
            pltpu.VMEM(large[0].shape, BF16),
            pltpu.VMEM(large[1].shape, BF16),
            pltpu.VMEM(large[2].shape, BF16),
            pltpu.VMEM(large[3].shape, BF16),
            pltpu.VMEM(large[4].shape, BF16),
            pltpu.VMEM(large[5].shape, BF16),
            pltpu.VMEM(large[6].shape, BF16),
            pltpu.VMEM(large[7].shape, BF16),
            pltpu.VMEM(large[8].shape, BF16),
            pltpu.VMEM(large[9].shape, BF16),
            pltpu.VMEM((n_tp, hidden, chunk), BF16),
            pltpu.VMEM(large[11].shape, BF16),
            pltpu.SemaphoreType.DMA((12 + n_tp,)),
            pltpu.VMEM((n_ep, rows, depth), BF16),
            pltpu.VMEM((n_ep, rows, depth), BF16),
            pltpu.SemaphoreType.DMA((n_ep,)),
            pltpu.SemaphoreType.DMA((n_ep,)),
            pltpu.VMEM((8, 128), F32),
            pltpu.VMEM((ratio, 8, 128), F32),
            pltpu.SemaphoreType.DMA((n_ep,)),
            pltpu.SemaphoreType.DMA((ratio,)),
            pltpu.VMEM((n_ep, rows, depth), BF16),
            pltpu.VMEM((ratio, rows, depth), BF16),
            pltpu.SemaphoreType.DMA((n_ep,)),
            pltpu.SemaphoreType.DMA((ratio,)),
            pltpu.VMEM((3, 2, half, rows, hidden), F32),
            pltpu.VMEM((3, half, rows, hidden), F32),
            pltpu.SemaphoreType.DMA((3,)),
            pltpu.SemaphoreType.DMA((3,)),
            pltpu.VMEM((2, half, rows, hidden), F32),
            pltpu.VMEM((2, half, rows, hidden), F32),
            pltpu.SemaphoreType.DMA((2, half)),
            pltpu.SemaphoreType.DMA((2, half)),
            pltpu.VMEM((half, rows, hidden), BF16),
            pltpu.VMEM((half, rows, hidden), BF16),
            pltpu.SemaphoreType.DMA((half,)),
            pltpu.SemaphoreType.DMA((half,)),
            pltpu.VMEM((rows, heads, size), F32),
            pltpu.VMEM((rows, heads, size), F32),
            pltpu.VMEM((rows, heads, size), F32),
            pltpu.VMEM((rows, heads, size), F32),
            pltpu.VMEM((rows, heads, span), F32),
            pltpu.VMEM((rows, heads, size), F32),
            pltpu.VMEM((rows, hidden), BF16),
            pltpu.VMEM((n_ep, rows, hidden), BF16),
            pltpu.SemaphoreType.DMA((n_ep,)),
            pltpu.SemaphoreType.DMA((n_ep,)),
            pltpu.VMEM((n_tp, ratio, rows, depth), F32),
            pltpu.VMEM((n_tp, ratio, rows, depth), F32),
            pltpu.SemaphoreType.DMA((n_tp,)),
            pltpu.SemaphoreType.DMA((n_tp,)),
            pltpu.VMEM((n_tp, ratio, rows, depth), BF16),
            pltpu.VMEM((ratio, rows, depth), BF16),
            pltpu.SemaphoreType.DMA((n_tp,)),
            pltpu.SemaphoreType.DMA((n_tp,)),
            pltpu.VMEM((ratio, rows, depth), BF16),
            pltpu.SemaphoreType.DMA((n_ep,)),
            pltpu.SemaphoreType.DMA((ratio,)),
            pltpu.VMEM((n_ep, ratio, slots, depth), BF16),
            pltpu.VMEM((n_tp, n_ep, ratio, slots, depth), BF16),
            pltpu.SemaphoreType.DMA((n_ep,)),
            pltpu.SemaphoreType.DMA((n_ep,)),
            pltpu.SemaphoreType.DMA((n_tp,)),
            pltpu.SemaphoreType.DMA((n_tp,)),
            pltpu.VMEM((n_tp * ratio * slots, model), BF16),
            pltpu.VMEM((n_ep, 1, depth), F32),
            pltpu.VMEM((2, half, rows, 2 * hidden + 128), F32),
            pltpu.VMEM((half, rows, 2 * hidden + 128), F32),
            pltpu.SemaphoreType.DMA((1,)),
            pltpu.SemaphoreType.DMA((1,)),
            pltpu.VMEM((half, rows, 2 * hidden + 128), BF16),
            pltpu.VMEM((half, rows, 2 * hidden + 128), BF16),
            pltpu.SemaphoreType.DMA((half,)),
            pltpu.SemaphoreType.DMA((half,)),
            pltpu.VMEM((rows, hidden), BF16),
            pltpu.VMEM((n_ep, rows, hidden), BF16),
            pltpu.SemaphoreType.DMA((n_ep,)),
            pltpu.SemaphoreType.DMA((n_ep,)),
            pltpu.VMEM((n_tp, n_ep * slots, chunk), BF16),
            pltpu.VMEM((n_tp, n_ep * slots, chunk), BF16),
            pltpu.SemaphoreType.DMA((n_tp,)),
            pltpu.SemaphoreType.DMA((n_tp,)),
            pltpu.VMEM((n_ep, slots, chunk), BF16),
            pltpu.VMEM((n_ep, slots, chunk), BF16),
            pltpu.SemaphoreType.DMA((n_ep,)),
            pltpu.SemaphoreType.DMA((n_ep,)),
            pltpu.VMEM((n_ep, rows, depth), BF16),
            pltpu.VMEM((n_ep, rows, depth), BF16),
            pltpu.SemaphoreType.DMA((n_ep,)),
            pltpu.SemaphoreType.DMA((n_ep,)),
            pltpu.VMEM((n_tp, ratio, rows, depth), BF16),
            pltpu.SemaphoreType.DMA((n_ep,)),
            pltpu.SemaphoreType.DMA((n_tp, ratio)),
            pltpu.VMEM((rows, chunk), F32),
            pltpu.VMEM((rows, chunk), BF16),
            pltpu.VMEM((n_tp, rows, chunk), BF16),
            pltpu.SemaphoreType.DMA((n_tp,)),
            pltpu.SemaphoreType.DMA((n_tp,)),
        ],
        compiler_params=pltpu.CompilerParams(
            collective_id=0, has_side_effects=True, vmem_limit_bytes=60 * 1024 * 1024
        ),
    )(*scalars, *small, *large)


def shards(
    tokens,
    attn_gain,
    query_weight,
    key_weight,
    value_weight,
    forget_weight,
    forget_bias,
    cache_keys,
    cache_values,
    cache_gates,
    lengths,
    output_weight,
    ffn_gain,
    dense_gate_proj,
    dense_up_proj,
    dense_down_proj,
    dense_mix,
    expert_ids,
    group_prob,
    pair_prob,
    expert_gate,
    expert_up,
    expert_down,
):
    seq_count = tokens.shape[0]
    n_ep = lax.axis_size("ep")
    n_tp = lax.axis_size("tp")
    expert_count = n_ep * expert_gate.shape[0]
    capacity = max(4 * seq_count // expert_count, 8)
    model = (1, tokens.shape[1])
    return layer(
        n_ep,
        n_tp,
        capacity,
        (forget_bias.reshape(1, -1), lengths.reshape(1, -1)),
        (
            tokens,
            attn_gain.reshape(model),
            forget_weight.T,
            cache_gates,
            ffn_gain.reshape(model),
            ffn_gain.reshape(n_ep, 1, -1),
            dense_mix.reshape(-1, 128),
            expert_ids.T,
            group_prob.reshape(1, -1),
            pair_prob.T,
        ),
        (
            query_weight,
            key_weight,
            value_weight,
            cache_keys,
            cache_values,
            output_weight,
            dense_gate_proj,
            dense_up_proj,
            expert_gate,
            expert_up,
            expert_down,
            dense_down_proj,
        ),
    )


def solution(mesh):
    return jax.shard_map(
        shards,
        mesh=mesh,
        in_specs=(
            P("ep", None),
            P(),
            P("ep", "tp"),
            P("ep", "tp"),
            P("ep", "tp"),
            P(None, "tp"),
            P("tp"),
            P("ep", "tp", None, None),
            P("ep", "tp", None, None),
            P("ep", "tp", None),
            P("ep"),
            P("tp", "ep"),
            P(),
            P("ep", "tp"),
            P("ep", "tp"),
            P("tp", "ep"),
            P(),
            P("ep", None),
            P("ep"),
            P("ep", None),
            P("ep", None, "tp"),
            P("ep", None, "tp"),
            P("ep", "tp", None),
        ),
        out_specs=P("ep", None),
        check_vma=False,
    )
```

```python
import functools
import math

import jax
import jax.numpy as jnp
from jax import lax
from jax.experimental import pallas as pl
from jax.experimental.pallas import tpu as pltpu
from jax.sharding import PartitionSpec as P

EPSILON = 1e-06


def rms_scale(values, norm_gain):
    widened = values.astype(jnp.float32)
    return (
        widened
        * lax.rsqrt(jnp.mean(widened * widened, axis=-1, keepdims=True) + EPSILON)
        * norm_gain
    )


MESH = pl.DeviceIdType.MESH
F32 = jnp.float32
BF16 = jnp.bfloat16


def flip(me, step):
    bit = 1
    while bit <= step:
        if step & bit:
            me = me + bit - 2 * bit * lax.rem(me // bit, 2)
        bit *= 2
    return me


def toward(me, step, count):
    return flip(me, step) if count & (count - 1) == 0 else lax.rem(me + step, count)


def origin(me, step, count):
    return flip(me, step) if count & (count - 1) == 0 else lax.rem(me + count - step, count)


def far_first(count):
    return range(count - 1, 0, -1)


def remote(source, place, send_sem, recv_sem, device):
    return pltpu.make_async_remote_copy(
        src_ref=source,
        dst_ref=place,
        send_sem=send_sem,
        recv_sem=recv_sem,
        device_id=device,
        device_id_type=MESH,
    )


def fan_out(axis, count, me, source_of, landing, send_sem, recv_sem):
    copies = []
    for step in far_first(count):
        target = toward(me, step, count)
        copy = remote(
            source_of(target),
            landing.at[me],
            send_sem.at[step],
            recv_sem.at[me],
            {axis: target},
        )
        copy.start()
        copies.append(copy)
    return copies


def arrive(axis, source, place, send_sem, recv_sem):
    remote(place, place, send_sem, recv_sem, {axis: source}).wait_recv()


def collect(axis, count, me, landing, send_sem, recv_sem):
    for step in range(1, count):
        source = origin(me, step, count)
        arrive(axis, source, landing.at[source], send_sem.at[step], recv_sem.at[source])


def total_of(ref, count):
    total = ref[0].astype(F32)
    for index in range(1, count):
        total = total + ref[index].astype(F32)
    return total


def dot32(left, right):
    return jnp.dot(left, right, preferred_element_type=F32)


def silu(values):
    return values / (1.0 + jnp.exp(-values))


def chip_fan(axis, half, me, source_of, landing, send_sem, recv_sem):
    chip, core = me // 2, lax.rem(me, 2)
    copies = []
    for step in far_first(half):
        target = toward(chip, step, half)
        copy = remote(
            source_of(target),
            landing.at[chip],
            send_sem.at[step],
            recv_sem.at[chip],
            {axis: target * 2 + core},
        )
        copy.start()
        copies.append(copy)
    return copies


def chip_collect(axis, half, me, landing, send_sem, recv_sem):
    chip, core = me // 2, lax.rem(me, 2)
    for step in range(1, half):
        source = origin(chip, step, half)
        arrive(
            axis, source * 2 + core, landing.at[source], send_sem.at[step], recv_sem.at[source]
        )


def pick(one_hot, held):
    return lax.dot_general(
        one_hot, held, (((0,), (0,)), ((), ())), preferred_element_type=F32
    )


def slot_tables(ids, experts, slots):
    rows = ids.shape[1]
    row_at = lax.broadcasted_iota(jnp.int32, (rows, rows), 0)
    row_to = lax.broadcasted_iota(jnp.int32, (rows, rows), 1)
    expert_at = lax.broadcasted_iota(jnp.int32, (experts, rows), 0).astype(F32)
    slot_at = lax.broadcasted_iota(jnp.int32, (slots, rows), 0).astype(F32)
    first = ids[0:1, :] == expert_at
    second = ids[1:2, :] == expert_at
    hits = (first | second).astype(F32).astype(BF16)
    earlier = (row_at < row_to).astype(F32).astype(BF16)
    ranks = dot32(hits, earlier)
    tables = []
    for chosen in (first, second):
        place = jnp.where(chosen, ranks, -1.0)
        tables.append(
            jnp.concatenate(
                [
                    (place[expert : expert + 1, :] == slot_at).astype(F32)
                    for expert in range(experts)
                ],
                axis=0,
            )
        )
    return tables


def route_columns(group_prob, pair_prob):
    rows = pair_prob.shape[1]
    row_at = lax.broadcasted_iota(jnp.int32, (rows, rows), 0)
    row_to = lax.broadcasted_iota(jnp.int32, (rows, rows), 1)
    probs = pair_prob[...]
    shares = group_prob[...] * probs / (probs[0:1, :] + probs[1:2, :])
    return [
        jnp.sum(jnp.where(row_at == row_to, shares[k : k + 1, :], 0.0), axis=-1, keepdims=True)
        for k in range(2)
    ]


def layer_kernel(
    n_ep,
    n_tp,
    forget_bias_in,
    lengths_in,
    tokens_in,
    attn_gain_in,
    forget_rows_in,
    gates_in,
    gain_parts_in,
    dense_mix_in,
    expert_ids_in,
    group_prob_in,
    pair_prob_in,
    query_weight,
    key_weight,
    value_weight,
    output_weight,
    dense_gate,
    dense_up,
    dense_down,
    keys,
    values,
    expert_gate,
    expert_up,
    expert_down,
    out,
    forget_bias,
    lengths,
    tokens,
    attn_gain,
    forget_rows,
    gates,
    gain_parts,
    dense_mix,
    expert_ids,
    group_prob,
    pair_prob,
    small_sem,
    query_held,
    key_held,
    value_held,
    output_held,
    dense_gate_held,
    dense_up_held,
    dense_down_held,
    keys_held,
    values_held,
    expert_gate_held,
    expert_up_held,
    expert_down_held,
    load_sem,
    weight_ss,
    weight_rs,
    norm_send,
    norm_land,
    norm_ss,
    norm_rs,
    ids_send,
    ids_land,
    ids_ss,
    ids_rs,
    token_send,
    token_land,
    token_ss,
    token_rs,
    part_kept,
    part_send,
    part_land,
    part_ss,
    part_rs,
    query_rows,
    key_rows,
    value_rows,
    forget_logs,
    scores,
    mixed,
    attended,
    att_land,
    att_ss,
    att_rs,
    head_send,
    head_land,
    head_ss,
    head_rs,
    res_send,
    res_land,
    res_ss,
    res_rs,
    own_land,
    own_ss,
    own_rs,
    slot_send,
    slot_land,
    slot_ss,
    slot_rs,
    pass_ss,
    pass_rs,
    ffn_rows,
    mix_parts,
    dense_send,
    dense_land,
    dense_ss,
    dense_rs,
    hidden_land,
    hidden_send,
    hidden_ss,
    hidden_rs,
    expert_send,
    expert_land,
    expert_ss,
    expert_rs,
    back_send,
    back_land,
    back_ss,
    back_rs,
    tail_send,
    tail_land,
    tail_ss,
    tail_rs,
    out_send,
    out_land,
    out_ss,
    out_rs,
    store_sem,
):
    me = lax.axis_index("ep")
    me_tp = lax.axis_index("tp")
    barrier = pltpu.get_barrier_semaphore()
    half = n_ep // 2
    chip, core = me // 2, lax.rem(me, 2)
    spreads = chip == me_tp

    def greet(axis, mine, count):
        def signal(step, carry):
            pl.semaphore_signal(
                barrier,
                inc=1,
                device_id={axis: lax.rem(mine + step, count)},
                device_id_type=MESH,
            )
            return carry

        lax.fori_loop(1, count, signal, 0, unroll=count <= 8)

    greet("ep", me, n_ep)
    greet("tp", me_tp, n_tp)
    small_loads = [
        pltpu.make_async_copy(source, place, small_sem.at[index])
        for index, (source, place) in enumerate(
            (
                (tokens_in, tokens),
                (attn_gain_in, attn_gain),
                (expert_ids_in, expert_ids),
                (forget_bias_in, forget_bias),
                (forget_rows_in, forget_rows),
                (group_prob_in, group_prob),
                (pair_prob_in, pair_prob),
                (dense_mix_in, dense_mix),
                (gain_parts_in, gain_parts),
                (lengths_in, lengths),
                (gates_in, gates),
            )
        )
    ]
    for load in small_loads:
        load.start()
    rows, model = tokens.shape
    depth, hidden = query_weight.shape
    heads, span, size = keys.shape[1:]
    slots = slot_send.shape[1]
    chunk = model // n_tp
    cols = 2 * depth
    wide = 2 * hidden
    shared = (query_held, key_held, value_held, output_held, dense_gate_held, dense_up_held, dense_down_held)
    sources = [query_weight, key_weight, value_weight, output_weight, dense_gate, dense_up, dense_down, keys, values, expert_gate.at[0], expert_up.at[0]]
    places = [held.at[core] for held in shared]
    places += [keys_held, values_held, expert_gate_held, expert_up_held]
    for index in range(n_tp):
        sources.append(expert_down.at[0, :, pl.ds(index * chunk, chunk)])
        places.append(expert_down_held.at[index])
    loads = [
        pltpu.make_async_copy(source, place, load_sem.at[index])
        for index, (source, place) in enumerate(zip(sources, places))
    ]
    for load in loads[: len(shared)]:
        load.start()
    gifts = [
        remote(
            held.at[core],
            held.at[core],
            weight_ss.at[index],
            weight_rs.at[index],
            {"ep": me + 1 - 2 * core},
        )
        for index, held in enumerate(shared)
    ]

    for load in small_loads[:3]:
        load.wait()
    normed = rms_scale(tokens[...], attn_gain[...])
    for index in range(half):
        norm_send[index] = normed[:, index * cols : (index + 1) * cols].astype(BF16)
        token_send[index] = tokens[:, index * cols : (index + 1) * cols]
    ids = expert_ids[...].astype(F32)
    ids_send[0:2, 0:rows] = ids
    pl.semaphore_wait(barrier, n_ep + n_tp - 2)

    sent = chip_fan("ep", half, me, lambda t: norm_send.at[t], norm_land, norm_ss, norm_rs)
    norm_land[chip] = norm_send[chip]
    for load in loads[len(shared) :]:
        load.start()
    for index in range(len(shared)):
        loads[index].wait()
        gifts[index].start()

    def row_copies(source_of, landing, send_sem, recv_sem):
        return [
            remote(
                source_of(toward(chip, step, half)),
                landing,
                send_sem.at[step],
                recv_sem.at[0],
                {"ep": toward(chip, step, half) * 2 + core},
            )
            for step in far_first(half)
        ]

    def row_arrival(landing, send_sem, recv_sem):
        @pl.when(jnp.logical_not(spreads))
        def _():
            arrive("ep", me_tp * 2 + core, landing, send_sem.at[0], recv_sem.at[0])

    spread_early = row_copies(lambda t: token_send.at[t], token_land, token_ss, token_rs)
    spread_early += row_copies(lambda t: ids_send, ids_land, ids_ss, ids_rs)

    @pl.when(spreads)
    def _():
        for copy in spread_early:
            copy.start()
        token_land[...] = token_send[chip]
        ids_land[...] = ids_send[...]

    chip_collect("ep", half, me, norm_land, norm_ss, norm_rs)
    joined = norm_land[...].reshape(half * rows, cols)
    for index in range(3):
        gifts[index].wait_recv()
        product = dot32(joined, shared[index][...].reshape(cols, hidden)).reshape(
            half, rows, hidden
        )
        part_send[index] = product.astype(BF16)
        sent += chip_fan(
            "ep",
            half,
            me,
            lambda t: part_send.at[index, t],
            part_land.at[index],
            part_ss.at[index],
            part_rs.at[index],
        )
        part_kept[index] = product
    for load in small_loads[3:]:
        load.wait()
    normed_wide = normed.astype(BF16).astype(F32)
    for head in range(heads):
        logit = forget_bias[0, head] + jnp.sum(
            normed_wide * forget_rows[head : head + 1, :].astype(F32), axis=-1, keepdims=True
        )
        forget_log = jnp.minimum(logit, 0.0) - jnp.log1p(jnp.exp(-jnp.abs(logit)))
        forget_logs[:, head, :] = jnp.broadcast_to(forget_log, (rows, size))
    mix_lanes = dense_mix.shape[1]
    mix_wide = dense_mix[...].astype(F32)
    for at in range(0, model, mix_lanes):
        start = at % cols
        mix_parts[at // cols, :, start : start + mix_lanes] = mix_wide[
            at // mix_lanes : at // mix_lanes + 1, :
        ]
    first_table, second_table = slot_tables(ids, n_ep, slots)
    to_first, to_second = first_table.astype(BF16), second_table.astype(BF16)
    first_route, second_route = route_columns(group_prob, pair_prob)
    row_arrival(ids_land, ids_ss, ids_rs)
    tables = slot_tables(ids_land[0:2, 0:rows], n_ep, slots)
    dispatch = (tables[0] + tables[1]).astype(BF16)
    row_arrival(token_land, token_ss, token_rs)

    def reduced(index):
        chip_collect("ep", half, me, part_land.at[index], part_ss.at[index], part_rs.at[index])
        total = part_kept[index, chip]
        for step in range(1, half):
            total = total + part_land[index, origin(chip, step, half)].astype(F32)
        return total.astype(BF16).astype(F32)

    summed = reduced(0)
    for head in range(heads):
        query_rows[:, head, :] = summed[:, head * size : (head + 1) * size]

    scale = 1.0 / math.sqrt(size)
    loads[7].wait()
    loads[8].wait()

    def score_step(seq, carry):
        for head in range(heads):
            query = query_rows[seq, head : head + 1, :].astype(BF16)
            scores[seq, head : head + 1, :] = lax.dot_general(
                query,
                keys_held[seq, head],
                (((1,), (1,)), ((), ())),
                preferred_element_type=F32,
            )
        return carry

    lax.fori_loop(0, rows, score_step, 0, unroll=4)
    summed = reduced(1)
    for head in range(heads):
        key_rows[:, head, :] = summed[:, head * size : (head + 1) * size]
    positions = lax.broadcasted_iota(jnp.int32, (rows, heads, span), 2)
    sequences = lax.broadcasted_iota(jnp.int32, (rows, heads, size), 0)
    live_wide = jnp.zeros((rows, heads, size), jnp.int32)
    for seq in range(rows):
        live_wide = jnp.where(sequences == seq, lengths[0, seq], live_wide)
    lives = live_wide[:, :, 0:1]
    gate_all = gates[...]
    last_gate = jnp.sum(jnp.where(positions == lives - 1, gate_all, 0.0), axis=-1, keepdims=True)
    gate_now = last_gate + forget_logs[:, :, 0:1]
    score_all = scores[...] * scale + gate_now - gate_all
    score_all = jnp.where(positions < lives, score_all, -jnp.inf)
    own_score = jnp.sum(query_rows[...] * key_rows[...], axis=-1, keepdims=True) * scale
    row_top = jnp.maximum(jnp.max(score_all, axis=-1, keepdims=True), own_score)
    raised = jnp.exp(score_all - row_top)
    own_raised = jnp.exp(own_score - row_top)
    totals = jnp.sum(raised, axis=-1, keepdims=True) + own_raised
    scores[...] = raised / totals
    own_prob = (own_raised / totals).astype(BF16).astype(F32)

    def value_step(seq, carry):
        for head in range(heads):
            weight = scores[seq, head : head + 1, :].astype(BF16)
            mixed[seq, head : head + 1, :] = dot32(weight, values_held[seq, head])
        return carry

    lax.fori_loop(0, rows, value_step, 0, unroll=4)
    value_sum = reduced(2)
    for head in range(heads):
        value_rows[:, head, :] = value_sum[:, head * size : (head + 1) * size]
    mixed[...] = mixed[...] + own_prob * value_rows[...]
    for head in range(heads):
        attended[:, head * size : (head + 1) * size] = mixed[:, head, :].astype(BF16)

    sent += chip_fan("ep", half, me, lambda t: attended, att_land, att_ss, att_rs)
    att_land[chip] = attended[...]
    gifts[3].wait_recv()
    chip_collect("ep", half, me, att_land, att_ss, att_rs)
    joined = att_land[...].reshape(half * rows, hidden)
    for side in range(2):
        head_send[:, :, side * depth : (side + 1) * depth] = dot32(
            joined, output_held[side]
        ).reshape(n_tp, rows, depth)
    sent += fan_out("tp", n_tp, me_tp, lambda t: head_send.at[t], head_land, head_ss, head_rs)
    head_land[me_tp] = head_send[me_tp]
    collect("tp", n_tp, me_tp, head_land, head_ss, head_rs)
    residual = (token_land[...].astype(F32) + total_of(head_land, n_tp)).astype(BF16)
    res_send[...] = residual
    sent += fan_out("tp", n_tp, me_tp, lambda t: res_send, res_land, res_ss, res_rs)
    slot_send[...] = dot32(dispatch, residual).reshape(n_ep, slots, cols).astype(BF16)

    def slot_place(source):
        return slot_land.at[me_tp, source // 2, lax.rem(source, 2)]

    for step in far_first(n_ep):
        target = toward(me, step, n_ep)
        copy = remote(
            slot_send.at[target],
            slot_place(me),
            slot_ss.at[step],
            slot_rs.at[me],
            {"ep": target},
        )
        copy.start()
        sent.append(copy)
    slot_land[me_tp, chip, core] = slot_send[me]
    res_land[me_tp] = residual

    def forward(source):
        for step in far_first(n_tp):
            remote(
                slot_place(source),
                slot_place(source),
                pass_ss.at[step],
                pass_rs.at[me_tp],
                {"tp": toward(me_tp, step, n_tp)},
            ).start()

    def relay(step):
        source = origin(me, step, n_ep)
        arrive("ep", source, slot_place(source), slot_ss.at[step], slot_rs.at[source])
        forward(source)

    forward(me)
    early = min(4, n_ep)
    for step in range(1, early):
        relay(step)

    collect("tp", n_tp, me_tp, res_land, res_ss, res_rs)
    held = res_land[...].reshape(half * rows, cols).astype(F32)
    dense_rows = (held * gain_parts[chip]).astype(BF16)
    for index, weight in ((4, dense_gate_held), (5, dense_up_held)):
        gifts[index].wait_recv()
        start = (index - 4) * hidden
        dense_send[:, :, start : start + hidden] = (
            dot32(dense_rows, weight[...].reshape(cols, hidden))
            .reshape(half, rows, hidden)
            .astype(BF16)
        )
    squares = jnp.sum(held * held, axis=-1, keepdims=True)
    mixes = jnp.sum(dense_rows.astype(F32) * mix_parts[chip], axis=-1, keepdims=True)
    lane_at = lax.broadcasted_iota(jnp.int32, (half * rows, 128), 1)
    sums = jnp.where(lax.rem(lane_at, 2) == 0, squares, mixes)
    coarse = sums.astype(BF16).astype(F32)
    dense_send[:, :, wide:] = (
        jnp.where(lane_at < 2, coarse, sums - coarse).astype(BF16).reshape(half, rows, 128)
    )
    sent += chip_fan("ep", half, me, lambda t: dense_send.at[t], dense_land, dense_ss, dense_rs)
    dense_land[chip] = dense_send[chip]
    owner_copies = row_copies(lambda t: res_land.at[t], own_land, own_ss, own_rs)

    @pl.when(spreads)
    def _():
        for copy in owner_copies:
            copy.start()
        own_land[...] = res_land[chip]

    for step in range(early, n_ep):
        relay(step)

    for step in range(1, n_tp):
        source = origin(me_tp, step, n_tp)
        arrive("tp", source, slot_land.at[source], pass_ss.at[step], pass_rs.at[source])
    total_slots = n_ep * slots
    square = jnp.zeros((total_slots, cols), F32)
    for index in range(half):
        part = slot_land[:, index].astype(F32).reshape(total_slots, cols)
        square = square + part * part
    slot_scale = lax.rsqrt(jnp.sum(square, axis=-1, keepdims=True) / model + EPSILON)
    for index in range(half):
        part = slot_land[:, index].astype(F32).reshape(total_slots, cols)
        ffn_rows[:, index * cols : (index + 1) * cols] = (
            part * slot_scale * gain_parts[index]
        ).astype(BF16)
    for load in loads[9:]:
        load.wait()
    ffn_in = ffn_rows[...]
    expert_hidden = (
        silu(dot32(ffn_in, expert_gate_held[...])) * dot32(ffn_in, expert_up_held[...])
    ).astype(BF16)
    chip_collect("ep", half, me, dense_land, dense_ss, dense_rs)
    dense_sum = total_of(dense_land, half)
    sums = dense_sum[:, wide:]
    row_scale = lax.rsqrt((sums[:, 0:1] + sums[:, 2:3]) / model + EPSILON)
    mix = jax.nn.sigmoid((sums[:, 1:2] + sums[:, 3:4]) * row_scale)
    dense_pair = dense_sum[:, :wide] * row_scale
    hidden_send[...] = (silu(dense_pair[:, :hidden]) * dense_pair[:, hidden:]).astype(BF16)
    sent += chip_fan("ep", half, me, lambda t: hidden_send, hidden_land, hidden_ss, hidden_rs)
    hidden_land[chip] = hidden_send[...]

    for step in far_first(n_tp):
        target = toward(me_tp, step, n_tp)
        expert_send[target] = dot32(expert_hidden, expert_down_held[target]).astype(BF16)
        copy = remote(
            expert_send.at[target],
            expert_land.at[me_tp],
            expert_ss.at[step],
            expert_rs.at[me_tp],
            {"tp": target},
        )
        copy.start()
        sent.append(copy)
    expert_land[me_tp] = dot32(expert_hidden, expert_down_held[me_tp]).astype(BF16)

    gifts[6].wait_recv()
    chip_collect("ep", half, me, hidden_land, hidden_ss, hidden_rs)
    joined = hidden_land[...].reshape(half * rows, hidden)
    for side in range(2):
        tail_send[:, :, side * depth : (side + 1) * depth] = (
            dot32(joined, dense_down_held[side]).reshape(half, rows, depth).astype(BF16)
        )

    def tail_copy(target):
        return remote(
            tail_send.at[target],
            tail_land.at[me_tp],
            tail_ss.at[target],
            tail_rs.at[me_tp],
            {"ep": target * 2 + core, "tp": chip},
        )

    for step in range(half - 1, -1, -1):
        target = chip if step == 0 else toward(chip, step, half)
        if step:
            tail_copy(target).start()
        else:
            pl.when(jnp.logical_not(spreads))(lambda: tail_copy(chip).start())

    @pl.when(spreads)
    def _():
        tail_land[me_tp] = tail_send[chip]

    collect("tp", n_tp, me_tp, expert_land, expert_ss, expert_rs)
    expert_total = total_of(expert_land, n_tp)
    for index in range(n_ep):
        back_send[index] = expert_total[index * slots : (index + 1) * slots].astype(BF16)
    sent += fan_out("ep", n_ep, me, lambda t: back_send.at[t], back_land, back_ss, back_rs)
    back_land[me] = back_send[me]
    for copy in gifts:
        copy.wait_send()
    for copy in sent[: -(n_ep - 1)]:
        copy.wait_send()
    for step in range(1, n_tp):
        remote(
            slot_land.at[me_tp],
            slot_land.at[me_tp],
            pass_ss.at[step],
            pass_rs.at[me_tp],
            {"tp": toward(me_tp, step, n_tp)},
        ).wait_send()

    @pl.when(spreads)
    def _():
        for copy in spread_early + owner_copies:
            copy.wait_send()

    row_arrival(own_land, own_ss, own_rs)
    collect("ep", n_ep, me, back_land, back_ss, back_rs)
    back_rows = jnp.concatenate(
        [back_land[index].astype(F32) for index in range(n_ep)], axis=0
    ).astype(BF16)
    partial = (
        own_land[...].astype(F32)
        + first_route * pick(to_first, back_rows)
        + second_route * pick(to_second, back_rows)
    )
    for step in range(n_tp):
        source = me_tp if step == 0 else origin(me_tp, step, n_tp)

        def landed():
            remote(
                tail_land.at[source],
                tail_land.at[source],
                tail_ss.at[0],
                tail_rs.at[source],
                {"ep": me_tp * 2 + core, "tp": source},
            ).wait_recv()

        if step:
            landed()
        else:
            pl.when(jnp.logical_not(spreads))(landed)
    out_send[...] = (partial + mix * total_of(tail_land, n_tp)).astype(BF16)
    last = fan_out("tp", n_tp, me_tp, lambda t: out_send, out_land, out_ss, out_rs)

    def store(index, source):
        return pltpu.make_async_copy(
            source,
            out.at[:, pl.ds(pl.multiple_of(index * chunk, chunk), chunk)],
            store_sem.at[index],
        )

    store(me_tp, out_send).start()
    for copy in sent[-(n_ep - 1) :]:
        copy.wait_send()
    for step in range(half):
        target = chip if step == 0 else toward(chip, step, half)
        if step:
            tail_copy(target).wait_send()
        else:
            pl.when(jnp.logical_not(spreads))(lambda: tail_copy(chip).wait_send())
    for step in range(1, n_tp):
        source = origin(me_tp, step, n_tp)
        arrive("tp", source, out_land.at[source], out_ss.at[step], out_rs.at[source])
        store(source, out_land.at[source]).start()
    for copy in last:
        copy.wait_send()
    for step in range(1, n_tp):
        source = origin(me_tp, step, n_tp)
        store(source, out_land.at[source]).wait()
    store(me_tp, out_send).wait()


def layer(n_ep, n_tp, slots, small, large):
    rows, model = small[2].shape
    mix_shape = small[7].shape
    depth, hidden = large[0].shape
    keys = large[7]
    heads, span, size = keys.shape[1:]
    half = n_ep // 2
    chunk = model // n_tp
    cols = 2 * depth
    if half != n_tp:
        raise ValueError("unsupported mesh")
    hbm = pl.BlockSpec(memory_space=pltpu.HBM)
    return pl.pallas_call(
        functools.partial(layer_kernel, n_ep, n_tp),
        out_shape=jax.ShapeDtypeStruct((rows, model), BF16),
        in_specs=[hbm] * (len(small) + len(large)),
        out_specs=hbm,
        scratch_shapes=[
            pltpu.SMEM((1, heads), F32),
            pltpu.SMEM((1, rows), jnp.int32),
            pltpu.VMEM((rows, model), BF16),
            pltpu.VMEM((1, model), F32),
            pltpu.VMEM((heads, model), BF16),
            pltpu.VMEM((rows, heads, span), F32),
            pltpu.VMEM((half, 1, cols), F32),
            pltpu.VMEM(mix_shape, BF16),
            pltpu.VMEM((2, rows), jnp.int32),
            pltpu.VMEM((1, rows), F32),
            pltpu.VMEM((2, rows), F32),
            pltpu.SemaphoreType.DMA((11,)),
            pltpu.VMEM((2, depth, hidden), BF16),
            pltpu.VMEM((2, depth, hidden), BF16),
            pltpu.VMEM((2, depth, hidden), BF16),
            pltpu.VMEM((2, hidden, depth), BF16),
            pltpu.VMEM((2, depth, hidden), BF16),
            pltpu.VMEM((2, depth, hidden), BF16),
            pltpu.VMEM((2, hidden, depth), BF16),
            pltpu.VMEM(keys.shape, BF16),
            pltpu.VMEM(keys.shape, BF16),
            pltpu.VMEM((model, hidden), BF16),
            pltpu.VMEM((model, hidden), BF16),
            pltpu.VMEM((n_tp, hidden, chunk), BF16),
            pltpu.SemaphoreType.DMA((11 + n_tp,)),
            pltpu.SemaphoreType.DMA((7,)),
            pltpu.SemaphoreType.DMA((7,)),
            pltpu.VMEM((half, rows, cols), BF16),
            pltpu.VMEM((half, rows, cols), BF16),
            pltpu.SemaphoreType.DMA((half,)),
            pltpu.SemaphoreType.DMA((half,)),
            pltpu.VMEM((8, 128), F32),
            pltpu.VMEM((8, 128), F32),
            pltpu.SemaphoreType.DMA((half,)),
            pltpu.SemaphoreType.DMA((1,)),
            pltpu.VMEM((half, rows, cols), BF16),
            pltpu.VMEM((rows, cols), BF16),
            pltpu.SemaphoreType.DMA((half,)),
            pltpu.SemaphoreType.DMA((1,)),
            pltpu.VMEM((3, half, rows, hidden), F32),
            pltpu.VMEM((3, half, rows, hidden), BF16),
            pltpu.VMEM((3, half, rows, hidden), BF16),
            pltpu.SemaphoreType.DMA((3, half)),
            pltpu.SemaphoreType.DMA((3, half)),
            pltpu.VMEM((rows, heads, size), F32),
            pltpu.VMEM((rows, heads, size), F32),
            pltpu.VMEM((rows, heads, size), F32),
            pltpu.VMEM((rows, heads, size), F32),
            pltpu.VMEM((rows, heads, span), F32),
            pltpu.VMEM((rows, heads, size), F32),
            pltpu.VMEM((rows, hidden), BF16),
            pltpu.VMEM((half, rows, hidden), BF16),
            pltpu.SemaphoreType.DMA((half,)),
            pltpu.SemaphoreType.DMA((half,)),
            pltpu.VMEM((n_tp, rows, cols), F32),
            pltpu.VMEM((n_tp, rows, cols), F32),
            pltpu.SemaphoreType.DMA((n_tp,)),
            pltpu.SemaphoreType.DMA((n_tp,)),
            pltpu.VMEM((rows, cols), BF16),
            pltpu.VMEM((n_tp, rows, cols), BF16),
            pltpu.SemaphoreType.DMA((n_tp,)),
            pltpu.SemaphoreType.DMA((n_tp,)),
            pltpu.VMEM((rows, cols), BF16),
            pltpu.SemaphoreType.DMA((half,)),
            pltpu.SemaphoreType.DMA((1,)),
            pltpu.VMEM((n_ep, slots, cols), BF16),
            pltpu.VMEM((n_tp, half, 2, slots, cols), BF16),
            pltpu.SemaphoreType.DMA((n_ep,)),
            pltpu.SemaphoreType.DMA((n_ep,)),
            pltpu.SemaphoreType.DMA((n_tp,)),
            pltpu.SemaphoreType.DMA((n_tp,)),
            pltpu.VMEM((n_ep * slots, model), BF16),
            pltpu.VMEM((half, 1, cols), F32),
            pltpu.VMEM((half, rows, 2 * hidden + 128), BF16),
            pltpu.VMEM((half, rows, 2 * hidden + 128), BF16),
            pltpu.SemaphoreType.DMA((half,)),
            pltpu.SemaphoreType.DMA((half,)),
            pltpu.VMEM((half, rows, hidden), BF16),
            pltpu.VMEM((rows, hidden), BF16),
            pltpu.SemaphoreType.DMA((half,)),
            pltpu.SemaphoreType.DMA((half,)),
            pltpu.VMEM((n_tp, n_ep * slots, chunk), BF16),
            pltpu.VMEM((n_tp, n_ep * slots, chunk), BF16),
            pltpu.SemaphoreType.DMA((n_tp,)),
            pltpu.SemaphoreType.DMA((n_tp,)),
            pltpu.VMEM((n_ep, slots, chunk), BF16),
            pltpu.VMEM((n_ep, slots, chunk), BF16),
            pltpu.SemaphoreType.DMA((n_ep,)),
            pltpu.SemaphoreType.DMA((n_ep,)),
            pltpu.VMEM((half, rows, cols), BF16),
            pltpu.VMEM((n_tp, rows, cols), BF16),
            pltpu.SemaphoreType.DMA((half,)),
            pltpu.SemaphoreType.DMA((n_tp,)),
            pltpu.VMEM((rows, chunk), BF16),
            pltpu.VMEM((n_tp, rows, chunk), BF16),
            pltpu.SemaphoreType.DMA((n_tp,)),
            pltpu.SemaphoreType.DMA((n_tp,)),
            pltpu.SemaphoreType.DMA((n_tp,)),
        ],
        compiler_params=pltpu.CompilerParams(
            collective_id=0, has_side_effects=True, vmem_limit_bytes=60 * 1024 * 1024
        ),
    )(*small, *large)


def shards(
    tokens,
    attn_gain,
    query_weight,
    key_weight,
    value_weight,
    forget_weight,
    forget_bias,
    cache_keys,
    cache_values,
    cache_gates,
    lengths,
    output_weight,
    ffn_gain,
    dense_gate_proj,
    dense_up_proj,
    dense_down_proj,
    dense_mix,
    expert_ids,
    group_prob,
    pair_prob,
    expert_gate,
    expert_up,
    expert_down,
):
    seq_count = tokens.shape[0]
    n_ep = lax.axis_size("ep")
    n_tp = lax.axis_size("tp")
    expert_count = n_ep * expert_gate.shape[0]
    capacity = max(4 * seq_count // expert_count, 8)
    model = (1, tokens.shape[1])
    return layer(
        n_ep,
        n_tp,
        capacity,
        (
            forget_bias.reshape(1, -1),
            lengths.reshape(1, -1),
            tokens,
            attn_gain.reshape(model),
            forget_weight.T,
            cache_gates,
            ffn_gain.reshape(n_ep // 2, 1, -1),
            dense_mix.reshape(-1, 128),
            expert_ids.T,
            group_prob.reshape(1, -1),
            pair_prob.T,
        ),
        (
            query_weight,
            key_weight,
            value_weight,
            output_weight,
            dense_gate_proj,
            dense_up_proj,
            dense_down_proj,
            cache_keys,
            cache_values,
            expert_gate,
            expert_up,
            expert_down,
        ),
    )


def solution(mesh):
    return jax.shard_map(
        shards,
        mesh=mesh,
        in_specs=(
            P("ep", None),
            P(),
            P("ep", "tp"),
            P("ep", "tp"),
            P("ep", "tp"),
            P(None, "tp"),
            P("tp"),
            P("ep", "tp", None, None),
            P("ep", "tp", None, None),
            P("ep", "tp", None),
            P("ep"),
            P("tp", "ep"),
            P(),
            P("ep", "tp"),
            P("ep", "tp"),
            P("tp", "ep"),
            P(),
            P("ep", None),
            P("ep"),
            P("ep", None),
            P("ep", None, "tp"),
            P("ep", None, "tp"),
            P("ep", "tp", None),
        ),
        out_specs=P("ep", None),
        check_vma=False,
    )
```

```python
import functools
import math

import jax
import jax.numpy as jnp
from jax import lax
from jax.experimental import pallas as pl
from jax.experimental.pallas import tpu as pltpu
from jax.sharding import PartitionSpec as P

EPSILON = 1e-06


def rms_scale(values, norm_gain):
    widened = values.astype(jnp.float32)
    return (
        widened
        * lax.rsqrt(jnp.mean(widened * widened, axis=-1, keepdims=True) + EPSILON)
        * norm_gain
    )


MESH = pl.DeviceIdType.MESH
F32 = jnp.float32
BF16 = jnp.bfloat16


def flip(me, step):
    bit = 1
    while bit <= step:
        if step & bit:
            me = me + bit - 2 * bit * lax.rem(me // bit, 2)
        bit *= 2
    return me


def toward(me, step, count):
    return flip(me, step) if count & (count - 1) == 0 else lax.rem(me + step, count)


def origin(me, step, count):
    return flip(me, step) if count & (count - 1) == 0 else lax.rem(me + count - step, count)


def far_first(count):
    return range(count - 1, 0, -1)


def remote(source, place, send_sem, recv_sem, device):
    return pltpu.make_async_remote_copy(
        src_ref=source,
        dst_ref=place,
        send_sem=send_sem,
        recv_sem=recv_sem,
        device_id=device,
        device_id_type=MESH,
    )


def batch_of(landing, count, send_sem, recv_sem, device):
    blocks = landing.at[pl.ds(0, count)]
    return remote(blocks, blocks, send_sem.at[0], recv_sem.at[0], device)


def fan_out(axis, count, me, source_of, landing, send_sem, recv_sem):
    for step in far_first(count):
        target = toward(me, step, count)
        remote(
            source_of(target),
            landing.at[me],
            send_sem.at[0],
            recv_sem.at[0],
            {axis: target},
        ).start()
    return batch_of(landing, count - 1, send_sem, recv_sem, {axis: toward(me, 1, count)})


def arrive(axis, source, place, send_sem, recv_sem):
    remote(place, place, send_sem, recv_sem, {axis: source}).wait_recv()


def total_of(ref, count):
    total = ref[0].astype(F32)
    for index in range(1, count):
        total = total + ref[index].astype(F32)
    return total


def dot32(left, right):
    return jnp.dot(left, right, preferred_element_type=F32)


def silu(values):
    return values / (1.0 + jnp.exp(-values))


def chip_fan(axis, half, me, source_of, landing, send_sem, recv_sem):
    chip, core = me // 2, lax.rem(me, 2)
    for step in far_first(half):
        target = toward(chip, step, half)
        remote(
            source_of(target),
            landing.at[chip],
            send_sem.at[0],
            recv_sem.at[0],
            {axis: target * 2 + core},
        ).start()
    return batch_of(
        landing, half - 1, send_sem, recv_sem, {axis: toward(chip, 1, half) * 2 + core}
    )


def pick(one_hot, held):
    return lax.dot_general(
        one_hot, held, (((0,), (0,)), ((), ())), preferred_element_type=F32
    )


def slot_tables(ids, experts, slots):
    rows = ids.shape[1]
    row_at = lax.broadcasted_iota(jnp.int32, (rows, rows), 0)
    row_to = lax.broadcasted_iota(jnp.int32, (rows, rows), 1)
    expert_at = lax.broadcasted_iota(jnp.int32, (experts, rows), 0).astype(F32)
    slot_at = lax.broadcasted_iota(jnp.int32, (slots, rows), 0).astype(F32)
    first = ids[0:1, :] == expert_at
    second = ids[1:2, :] == expert_at
    hits = (first | second).astype(F32).astype(BF16)
    earlier = (row_at < row_to).astype(F32).astype(BF16)
    ranks = dot32(hits, earlier)
    tables = []
    for chosen in (first, second):
        place = jnp.where(chosen, ranks, -1.0)
        tables.append(
            jnp.concatenate(
                [
                    (place[expert : expert + 1, :] == slot_at).astype(F32)
                    for expert in range(experts)
                ],
                axis=0,
            )
        )
    return tables


def route_columns(group_prob, pair_prob):
    rows = pair_prob.shape[1]
    row_at = lax.broadcasted_iota(jnp.int32, (rows, rows), 0)
    row_to = lax.broadcasted_iota(jnp.int32, (rows, rows), 1)
    probs = pair_prob[...]
    shares = group_prob[...] * probs / (probs[0:1, :] + probs[1:2, :])
    return [
        jnp.sum(jnp.where(row_at == row_to, shares[k : k + 1, :], 0.0), axis=-1, keepdims=True)
        for k in range(2)
    ]


def layer_kernel(
    n_ep,
    n_tp,
    forget_bias_in,
    lengths_in,
    tokens_in,
    attn_gain_in,
    forget_rows_in,
    gates_in,
    gain_parts_in,
    dense_mix_in,
    expert_ids_in,
    group_prob_in,
    pair_prob_in,
    query_weight,
    key_weight,
    value_weight,
    output_weight,
    dense_gate,
    dense_up,
    dense_down,
    keys,
    values,
    expert_gate,
    expert_up,
    expert_down,
    out,
    forget_bias,
    lengths,
    tokens,
    attn_gain,
    forget_rows,
    gates,
    gain_parts,
    dense_mix,
    expert_ids,
    group_prob,
    pair_prob,
    small_sem,
    wide_held,
    tall_held,
    keys_held,
    values_held,
    expert_gate_held,
    expert_up_held,
    expert_down_held,
    load_sem,
    weight_ss,
    weight_rs,
    norm_send,
    norm_land,
    norm_ss,
    norm_rs,
    ids_send,
    ids_land,
    ids_ss,
    ids_rs,
    token_send,
    token_land,
    token_ss,
    token_rs,
    part_kept,
    part_send,
    part_land,
    part_ss,
    part_rs,
    query_flat,
    key_flat,
    value_flat,
    forget_flat,
    gate_flat,
    scores,
    mixed,
    attended,
    att_land,
    att_ss,
    att_rs,
    head_send,
    head_land,
    head_ss,
    head_rs,
    res_send,
    res_land,
    res_ss,
    res_rs,
    own_land,
    own_ss,
    own_rs,
    slot_send,
    slot_land,
    slot_ss,
    slot_rs,
    pass_ss,
    pass_rs,
    mix_parts,
    dense_send,
    dense_land,
    dense_ss,
    dense_rs,
    hidden_land,
    hidden_send,
    hidden_ss,
    hidden_rs,
    expert_send,
    expert_land,
    expert_ss,
    expert_rs,
    back_send,
    back_land,
    back_ss,
    back_rs,
    tail_send,
    tail_land,
    tail_ss,
    tail_rs,
    out_send,
    out_land,
    out_ss,
    out_rs,
    store_sem,
):
    me = lax.axis_index("ep")
    me_tp = lax.axis_index("tp")
    barrier = pltpu.get_barrier_semaphore()
    half = n_ep // 2
    chip, core = me // 2, lax.rem(me, 2)
    spreads = chip == me_tp

    def greet(axis, mine, count):
        def signal(step, carry):
            pl.semaphore_signal(
                barrier,
                inc=1,
                device_id={axis: lax.rem(mine + step, count)},
                device_id_type=MESH,
            )
            return carry

        lax.fori_loop(1, count, signal, 0, unroll=count <= 8)

    greet("ep", me, n_ep)
    greet("tp", me_tp, n_tp)
    small_loads = [
        pltpu.make_async_copy(source, place, small_sem.at[index])
        for index, (source, place) in enumerate(
            (
                (tokens_in, tokens),
                (attn_gain_in, attn_gain),
                (expert_ids_in, expert_ids),
                (forget_bias_in, forget_bias),
                (forget_rows_in, forget_rows),
                (group_prob_in, group_prob),
                (pair_prob_in, pair_prob),
                (dense_mix_in, dense_mix),
                (gain_parts_in, gain_parts),
                (lengths_in, lengths),
                (gates_in, gates),
            )
        )
    ]
    for small in small_loads:
        small.start()
    rows, model = tokens.shape
    depth, hidden = query_weight.shape
    heads, span, size = keys.shape[1:]
    slots = slot_send.shape[1]
    chunk = model // n_tp
    cols = 2 * depth
    wide = 2 * hidden
    loads = [
        pltpu.make_async_copy(source, place, load_sem.at[index])
        for source, place, index in (
            (query_weight, wide_held.at[core, 0], 0),
            (key_weight, wide_held.at[core, 1], 0),
            (value_weight, wide_held.at[core, 2], 0),
            (dense_gate, wide_held.at[core, 3], 0),
            (dense_up, wide_held.at[core, 4], 0),
            (output_weight, tall_held.at[core, 0], 1),
            (dense_down, tall_held.at[core, 1], 1),
            (keys, keys_held, 2),
            (values, values_held, 3),
            (expert_gate, expert_gate_held, 4),
            (expert_up, expert_up_held, 5),
        )
    ]
    loads += [
        pltpu.make_async_copy(
            expert_down.at[0, :, pl.ds(index * chunk, chunk)],
            expert_down_held.at[index],
            load_sem.at[6],
        )
        for index in range(n_tp)
    ]
    for load in loads[:7]:
        load.start()

    def loaded(place, index):
        pltpu.make_async_copy(place, place, load_sem.at[index]).wait()

    gifts = [
        remote(
            place,
            place,
            weight_ss.at[index],
            weight_rs.at[index],
            {"ep": me + 1 - 2 * core},
        )
        for index, place in enumerate(
            (
                wide_held.at[core, pl.ds(0, 3)],
                wide_held.at[core, pl.ds(3, 2)],
                tall_held.at[core],
            )
        )
    ]

    for small in small_loads[:3]:
        small.wait()
    normed = rms_scale(tokens[...], attn_gain[...])
    for index in range(half):
        norm_send[index] = normed[:, index * cols : (index + 1) * cols].astype(BF16)
        token_send[index] = tokens[:, index * cols : (index + 1) * cols]
    ids = expert_ids[...].astype(F32)
    ids_send[0, 0:2, 0:rows] = ids
    pl.semaphore_wait(barrier, n_ep + n_tp - 2)

    norm_batch = chip_fan("ep", half, me, lambda t: norm_send.at[t], norm_land, norm_ss, norm_rs)
    sent = [norm_batch]
    norm_land[chip] = norm_send[chip]
    loaded(wide_held.at[core], 0)
    gifts[0].start()
    gifts[1].start()
    for load in loads[7:]:
        load.start()
    loaded(tall_held.at[core], 1)
    gifts[2].start()

    def row_copies(source_of, landing, send_sem, recv_sem):
        return [
            remote(
                source_of(toward(chip, step, half)),
                landing,
                send_sem.at[0],
                recv_sem.at[0],
                {"ep": toward(chip, step, half) * 2 + core},
            )
            for step in far_first(half)
        ]

    def row_arrival(landing, send_sem, recv_sem):
        @pl.when(jnp.logical_not(spreads))
        def _():
            arrive("ep", me_tp * 2 + core, landing, send_sem.at[0], recv_sem.at[0])

    def row_batch(blocks, send_sem, recv_sem):
        other = {"ep": toward(chip, 1, half) * 2 + core}
        return batch_of(blocks, half - 1, send_sem, recv_sem, other)

    spread_early = row_copies(lambda t: token_send.at[t], token_land, token_ss, token_rs)
    spread_early += row_copies(lambda t: ids_send.at[0], ids_land.at[0], ids_ss, ids_rs)

    @pl.when(spreads)
    def _():
        for copy in spread_early:
            copy.start()
        token_land[...] = token_send[chip]
        ids_land[0] = ids_send[0]

    norm_batch.wait_recv()
    gifts[0].wait_recv()
    joined = norm_land[...].reshape(half * rows, cols)
    part_batches = []
    for index in range(3):
        product = dot32(joined, wide_held[:, index].reshape(cols, hidden)).reshape(
            half, rows, hidden
        )
        part_send[index] = product.astype(BF16)
        part_batches.append(
            chip_fan(
                "ep",
                half,
                me,
                lambda t: part_send.at[index, t],
                part_land.at[index],
                part_ss.at[index],
                part_rs.at[index],
            )
        )
        part_kept[index] = product
    sent += part_batches
    for small in small_loads[3:]:
        small.wait()
    normed_wide = normed.astype(BF16).astype(F32)
    for head in range(heads):
        logit = forget_bias[0, head] + jnp.sum(
            normed_wide * forget_rows[head : head + 1, :].astype(F32), axis=-1, keepdims=True
        )
        forget_log = jnp.minimum(logit, 0.0) - jnp.log1p(jnp.exp(-jnp.abs(logit)))
        block = slice(head * rows, (head + 1) * rows)
        forget_flat[block, :] = jnp.broadcast_to(forget_log, (rows, size))
        gate_flat[block, :] = gates[:, head, :]
    mix_lanes = dense_mix.shape[1]
    mix_wide = dense_mix[...].astype(F32)
    for at in range(0, model, mix_lanes):
        start = at % cols
        mix_parts[at // cols, :, start : start + mix_lanes] = mix_wide[
            at // mix_lanes : at // mix_lanes + 1, :
        ]
    first_table, second_table = slot_tables(ids, n_ep, slots)
    to_first, to_second = first_table.astype(BF16), second_table.astype(BF16)
    first_route, second_route = route_columns(group_prob, pair_prob)
    row_arrival(ids_land.at[0], ids_ss, ids_rs)
    tables = slot_tables(ids_land[0][0:2, 0:rows], n_ep, slots)
    dispatch = (tables[0] + tables[1]).astype(BF16)
    row_arrival(token_land, token_ss, token_rs)

    def reduced(index, place):
        part_batches[index].wait_recv()
        total = part_kept[index, chip]
        for step in range(1, half):
            total = total + part_land[index, origin(chip, step, half)].astype(F32)
        total = total.astype(BF16).astype(F32)
        for head in range(heads):
            place[head * rows : (head + 1) * rows, :] = total[:, head * size : (head + 1) * size]

    flat = heads * rows
    scale = 1.0 / math.sqrt(size)
    positions = lax.broadcasted_iota(jnp.int32, (flat, span), 1)
    sequences = lax.broadcasted_iota(jnp.int32, (rows, size), 0)
    live_wide = jnp.zeros((rows, size), jnp.int32)
    for seq in range(rows):
        live_wide = jnp.where(sequences == seq, lengths[0, seq], live_wide)
    lives = jnp.concatenate([live_wide] * heads, axis=0)[:, 0:1]
    gate_all = gate_flat[...]
    last_gate = jnp.sum(jnp.where(positions == lives - 1, gate_all, 0.0), axis=-1, keepdims=True)
    gate_flat[...] = jnp.where(
        positions < lives, last_gate + forget_flat[:, 0:1] - gate_all, -jnp.inf
    )
    loaded(keys_held, 2)
    loaded(values_held, 3)
    reduced(0, query_flat)
    turned = jnp.transpose(query_flat[...]).astype(BF16)
    column = lax.broadcasted_iota(jnp.int32, (size, flat), 1)
    spots = [(head, seq) for head in range(heads) for seq in range(rows)]
    query_wide = jnp.concatenate(
        [
            jnp.where(column == spot, turned.astype(F32), 0.0).astype(BF16)
            for spot in range(flat)
        ],
        axis=0,
    )
    keys_wide = jnp.concatenate([keys_held[seq, head] for head, seq in spots], axis=1)
    score_all = jnp.transpose(dot32(keys_wide, query_wide)) * scale + gate_flat[...]
    reduced(1, key_flat)
    own_score = jnp.sum(query_flat[...] * key_flat[...], axis=-1, keepdims=True) * scale
    row_top = jnp.maximum(jnp.max(score_all, axis=-1, keepdims=True), own_score)
    raised = jnp.exp(score_all - row_top)
    own_raised = jnp.exp(own_score - row_top)
    totals = jnp.sum(raised, axis=-1, keepdims=True) + own_raised
    scores[...] = raised / totals
    own_prob = (own_raised / totals).astype(BF16).astype(F32)

    def value_step(seq, carry):
        for head in range(heads):
            line = pl.ds(head * rows + seq, 1)
            mixed[line, :] = dot32(scores[line, :].astype(BF16), values_held[seq, head])
        return carry

    lax.fori_loop(0, rows, value_step, 0, unroll=4)
    reduced(2, value_flat)
    blended = (mixed[...] + own_prob * value_flat[...]).astype(BF16)
    for head in range(heads):
        attended[:, head * size : (head + 1) * size] = blended[head * rows : (head + 1) * rows]

    att_batch = chip_fan("ep", half, me, lambda t: attended, att_land, att_ss, att_rs)
    att_land[chip] = attended[...]
    gifts[2].wait_recv()
    att_batch.wait_recv()
    joined = att_land[...].reshape(half * rows, hidden)
    for side in range(2):
        head_send[:, :, side * depth : (side + 1) * depth] = dot32(
            joined, tall_held[side, 0]
        ).reshape(n_tp, rows, depth)
    head_batch = fan_out(
        "tp", n_tp, me_tp, lambda t: head_send.at[t], head_land, head_ss, head_rs
    )
    head_land[me_tp] = head_send[me_tp]
    head_batch.wait_recv()
    residual = (token_land[...].astype(F32) + total_of(head_land, n_tp)).astype(BF16)
    res_send[...] = residual
    res_batch = fan_out("tp", n_tp, me_tp, lambda t: res_send, res_land, res_ss, res_rs)
    slot_send[...] = dot32(dispatch, residual).reshape(n_ep, slots, cols).astype(BF16)

    def slot_place(source):
        return slot_land.at[me_tp, source // 2, lax.rem(source, 2)]

    for step in far_first(n_ep):
        target = toward(me, step, n_ep)
        remote(
            slot_send.at[target],
            slot_place(me),
            slot_ss.at[0],
            slot_rs.at[me],
            {"ep": target},
        ).start()
    sent += [att_batch, head_batch, res_batch]
    sent.append(
        batch_of(slot_send, n_ep - 1, slot_ss, slot_rs, {"ep": toward(me, 1, n_ep)})
    )
    slot_land[me_tp, chip, core] = slot_send[me]
    res_land[me_tp] = residual

    def forward(source):
        for step in far_first(n_tp):
            remote(
                slot_place(source),
                slot_place(source),
                pass_ss.at[0],
                pass_rs.at[source // 2],
                {"tp": toward(me_tp, step, n_tp)},
            ).start()

    def relay(step):
        source = origin(me, step, n_ep)
        arrive("ep", source, slot_place(source), slot_ss.at[0], slot_rs.at[source])
        forward(source)

    forward(me)
    res_batch.wait_recv()
    gifts[1].wait_recv()
    held = res_land[...].reshape(half * rows, cols).astype(F32)
    dense_rows = (held * gain_parts[chip]).astype(BF16)
    for index in range(2):
        start = index * hidden
        dense_send[:, :, start : start + hidden] = (
            dot32(dense_rows, wide_held[:, 3 + index].reshape(cols, hidden))
            .reshape(half, rows, hidden)
            .astype(BF16)
        )
    squares = jnp.sum(held * held, axis=-1, keepdims=True)
    mixes = jnp.sum(dense_rows.astype(F32) * mix_parts[chip], axis=-1, keepdims=True)
    lane_at = lax.broadcasted_iota(jnp.int32, (half * rows, 128), 1)
    sums = jnp.where(lax.rem(lane_at, 2) == 0, squares, mixes)
    coarse = sums.astype(BF16).astype(F32)
    dense_send[:, :, wide:] = (
        jnp.where(lane_at < 2, coarse, sums - coarse).astype(BF16).reshape(half, rows, 128)
    )
    dense_batch = chip_fan(
        "ep", half, me, lambda t: dense_send.at[t], dense_land, dense_ss, dense_rs
    )
    dense_land[chip] = dense_send[chip]
    owner_copies = row_copies(lambda t: res_land.at[t], own_land, own_ss, own_rs)

    @pl.when(spreads)
    def _():
        for copy in owner_copies:
            copy.start()
        own_land[...] = res_land[chip]

    for step in range(1, n_ep):
        relay(step)

    def hidden_step():
        dense_batch.wait_recv()
        dense_sum = total_of(dense_land, half)
        sums = dense_sum[:, wide:]
        row_scale = lax.rsqrt((sums[:, 0:1] + sums[:, 2:3]) / model + EPSILON)
        mix = jax.nn.sigmoid((sums[:, 1:2] + sums[:, 3:4]) * row_scale)
        dense_pair = dense_sum[:, :wide] * row_scale
        hidden_send[...] = (silu(dense_pair[:, :hidden]) * dense_pair[:, hidden:]).astype(BF16)
        hidden_batch = chip_fan(
            "ep", half, me, lambda t: hidden_send, hidden_land, hidden_ss, hidden_rs
        )
        hidden_land[chip] = hidden_send[...]
        return mix, hidden_batch

    total_slots = n_ep * slots
    square = jnp.zeros((total_slots, cols), F32)
    gate_part = jnp.zeros((total_slots, hidden), F32)
    up_part = jnp.zeros((total_slots, hidden), F32)
    loaded(expert_gate_held, 4)
    loaded(expert_up_held, 5)
    for step in range(half):
        if step == half - 1:
            mix, hidden_batch = hidden_step()
        source = chip if step == 0 else origin(chip, step, half)
        blocks = slot_land.at[pl.ds(0, n_tp - 1), source]
        remote(
            blocks,
            blocks,
            pass_ss.at[0],
            pass_rs.at[source],
            {"tp": toward(me_tp, 1, n_tp)},
        ).wait_recv()
        part = slot_land[:, source].astype(F32).reshape(total_slots, cols)
        square = square + part * part
        part = (part * gain_parts[source]).astype(BF16)
        gate_part = gate_part + dot32(part, expert_gate_held[source])
        up_part = up_part + dot32(part, expert_up_held[source])
    slot_scale = lax.rsqrt(jnp.sum(square, axis=-1, keepdims=True) / model + EPSILON)
    expert_hidden = (silu(gate_part * slot_scale) * (up_part * slot_scale)).astype(BF16)

    loaded(expert_down_held, 6)
    for step in far_first(n_tp):
        target = toward(me_tp, step, n_tp)
        expert_send[target] = dot32(expert_hidden, expert_down_held[target]).astype(BF16)
        remote(
            expert_send.at[target],
            expert_land.at[me_tp],
            expert_ss.at[0],
            expert_rs.at[0],
            {"tp": target},
        ).start()
    expert_batch = batch_of(
        expert_land, n_tp - 1, expert_ss, expert_rs, {"tp": toward(me_tp, 1, n_tp)}
    )
    expert_land[me_tp] = dot32(expert_hidden, expert_down_held[me_tp]).astype(BF16)

    sent += [dense_batch, hidden_batch, expert_batch]

    hidden_batch.wait_recv()
    joined = hidden_land[...].reshape(half * rows, hidden)
    for side in range(2):
        tail_send[:, :, side * depth : (side + 1) * depth] = (
            dot32(joined, tall_held[side, 1]).reshape(half, rows, depth).astype(BF16)
        )

    def tail_copy(target):
        return remote(
            tail_send.at[target],
            tail_land.at[me_tp],
            tail_ss.at[0],
            tail_rs.at[0],
            {"ep": target * 2 + core, "tp": chip},
        )

    for step in range(half - 1, -1, -1):
        target = chip if step == 0 else toward(chip, step, half)
        if step:
            tail_copy(target).start()
        else:
            pl.when(jnp.logical_not(spreads))(lambda: tail_copy(chip).start())

    @pl.when(spreads)
    def _():
        tail_land[me_tp] = tail_send[chip]

    expert_batch.wait_recv()
    expert_total = total_of(expert_land, n_tp)
    for index in range(n_ep):
        back_send[index] = expert_total[index * slots : (index + 1) * slots].astype(BF16)
    back_batch = fan_out(
        "ep", n_ep, me, lambda t: back_send.at[t], back_land, back_ss, back_rs
    )
    back_land[me] = back_send[me]
    for copy in gifts:
        copy.wait_send()
    for copy in sent:
        copy.wait_send()
    passed = slot_land.at[pl.ds(0, n_tp - 1)]
    remote(
        passed, passed, pass_ss.at[0], pass_rs.at[0], {"tp": toward(me_tp, 1, n_tp)}
    ).wait_send()

    @pl.when(spreads)
    def _():
        row_batch(token_send, token_ss, token_rs).wait_send()
        row_batch(ids_send, ids_ss, ids_rs).wait_send()
        row_batch(res_land, own_ss, own_rs).wait_send()

    row_arrival(own_land, own_ss, own_rs)
    back_batch.wait_recv()
    back_rows = jnp.concatenate(
        [back_land[index].astype(F32) for index in range(n_ep)], axis=0
    ).astype(BF16)
    partial = (
        own_land[...].astype(F32)
        + first_route * pick(to_first, back_rows)
        + second_route * pick(to_second, back_rows)
    )
    def tail_batch(blocks, count):
        return batch_of(blocks, count, tail_ss, tail_rs, {"ep": toward(me, 2, n_ep)})

    for landed, count in ((spreads, half - 1), (jnp.logical_not(spreads), half)):

        @pl.when(landed)
        def _():
            tail_batch(tail_land, count).wait_recv()

    out_send[...] = (partial + mix * total_of(tail_land, n_tp)).astype(BF16)
    out_land[me_tp] = out_send[...]
    out_batch = fan_out("tp", n_tp, me_tp, lambda t: out_send, out_land, out_ss, out_rs)
    back_batch.wait_send()
    for left, count in ((spreads, half - 1), (jnp.logical_not(spreads), half)):

        @pl.when(left)
        def _():
            tail_batch(tail_send, count).wait_send()

    out_batch.wait_recv()
    for index in range(n_tp):
        pltpu.make_async_copy(
            out_land.at[index], out.at[:, pl.ds(index * chunk, chunk)], store_sem.at[0]
        ).start()
    out_batch.wait_send()
    pltpu.make_async_copy(tokens, out, store_sem.at[0]).wait()


def layer(n_ep, n_tp, slots, small, large):
    rows, model = small[2].shape
    mix_shape = small[7].shape
    depth, hidden = large[0].shape
    keys = large[7]
    heads, span, size = keys.shape[1:]
    half = n_ep // 2
    chunk = model // n_tp
    cols = 2 * depth
    if half != n_tp:
        raise ValueError("unsupported mesh")
    hbm = pl.BlockSpec(memory_space=pltpu.HBM)
    return pl.pallas_call(
        functools.partial(layer_kernel, n_ep, n_tp),
        out_shape=jax.ShapeDtypeStruct((rows, model), BF16),
        in_specs=[hbm] * (len(small) + len(large)),
        out_specs=hbm,
        scratch_shapes=[
            pltpu.SMEM((1, heads), F32),
            pltpu.SMEM((1, rows), jnp.int32),
            pltpu.VMEM((rows, model), BF16),
            pltpu.VMEM((1, model), F32),
            pltpu.VMEM((heads, model), BF16),
            pltpu.VMEM((rows, heads, span), F32),
            pltpu.VMEM((half, 1, cols), F32),
            pltpu.VMEM(mix_shape, BF16),
            pltpu.VMEM((2, rows), jnp.int32),
            pltpu.VMEM((1, rows), F32),
            pltpu.VMEM((2, rows), F32),
            pltpu.SemaphoreType.DMA((11,)),
            pltpu.VMEM((2, 5, depth, hidden), BF16),
            pltpu.VMEM((2, 2, hidden, depth), BF16),
            pltpu.VMEM(keys.shape, BF16),
            pltpu.VMEM(keys.shape, BF16),
            pltpu.VMEM((half, cols, hidden), BF16),
            pltpu.VMEM((half, cols, hidden), BF16),
            pltpu.VMEM((n_tp, hidden, chunk), BF16),
            pltpu.SemaphoreType.DMA((7,)),
            pltpu.SemaphoreType.DMA((3,)),
            pltpu.SemaphoreType.DMA((3,)),
            pltpu.VMEM((half, rows, cols), BF16),
            pltpu.VMEM((half, rows, cols), BF16),
            pltpu.SemaphoreType.DMA((1,)),
            pltpu.SemaphoreType.DMA((1,)),
            pltpu.VMEM((half, 8, 128), F32),
            pltpu.VMEM((1, 8, 128), F32),
            pltpu.SemaphoreType.DMA((1,)),
            pltpu.SemaphoreType.DMA((1,)),
            pltpu.VMEM((half, rows, cols), BF16),
            pltpu.VMEM((rows, cols), BF16),
            pltpu.SemaphoreType.DMA((1,)),
            pltpu.SemaphoreType.DMA((1,)),
            pltpu.VMEM((3, half, rows, hidden), F32),
            pltpu.VMEM((3, half, rows, hidden), BF16),
            pltpu.VMEM((3, half, rows, hidden), BF16),
            pltpu.SemaphoreType.DMA((3, 1)),
            pltpu.SemaphoreType.DMA((3, 1)),
            pltpu.VMEM((heads * rows, size), F32),
            pltpu.VMEM((heads * rows, size), F32),
            pltpu.VMEM((heads * rows, size), F32),
            pltpu.VMEM((heads * rows, size), F32),
            pltpu.VMEM((heads * rows, span), F32),
            pltpu.VMEM((heads * rows, span), F32),
            pltpu.VMEM((heads * rows, size), F32),
            pltpu.VMEM((rows, hidden), BF16),
            pltpu.VMEM((half, rows, hidden), BF16),
            pltpu.SemaphoreType.DMA((1,)),
            pltpu.SemaphoreType.DMA((1,)),
            pltpu.VMEM((n_tp, rows, cols), F32),
            pltpu.VMEM((n_tp, rows, cols), F32),
            pltpu.SemaphoreType.DMA((1,)),
            pltpu.SemaphoreType.DMA((1,)),
            pltpu.VMEM((rows, cols), BF16),
            pltpu.VMEM((n_tp, rows, cols), BF16),
            pltpu.SemaphoreType.DMA((1,)),
            pltpu.SemaphoreType.DMA((1,)),
            pltpu.VMEM((rows, cols), BF16),
            pltpu.SemaphoreType.DMA((1,)),
            pltpu.SemaphoreType.DMA((1,)),
            pltpu.VMEM((n_ep, slots, cols), BF16),
            pltpu.VMEM((n_tp, half, 2, slots, cols), BF16),
            pltpu.SemaphoreType.DMA((1,)),
            pltpu.SemaphoreType.DMA((n_ep,)),
            pltpu.SemaphoreType.DMA((1,)),
            pltpu.SemaphoreType.DMA((half,)),
            pltpu.VMEM((half, 1, cols), F32),
            pltpu.VMEM((half, rows, 2 * hidden + 128), BF16),
            pltpu.VMEM((half, rows, 2 * hidden + 128), BF16),
            pltpu.SemaphoreType.DMA((1,)),
            pltpu.SemaphoreType.DMA((1,)),
            pltpu.VMEM((half, rows, hidden), BF16),
            pltpu.VMEM((rows, hidden), BF16),
            pltpu.SemaphoreType.DMA((1,)),
            pltpu.SemaphoreType.DMA((1,)),
            pltpu.VMEM((n_tp, n_ep * slots, chunk), BF16),
            pltpu.VMEM((n_tp, n_ep * slots, chunk), BF16),
            pltpu.SemaphoreType.DMA((1,)),
            pltpu.SemaphoreType.DMA((1,)),
            pltpu.VMEM((n_ep, slots, chunk), BF16),
            pltpu.VMEM((n_ep, slots, chunk), BF16),
            pltpu.SemaphoreType.DMA((1,)),
            pltpu.SemaphoreType.DMA((1,)),
            pltpu.VMEM((half, rows, cols), BF16),
            pltpu.VMEM((n_tp, rows, cols), BF16),
            pltpu.SemaphoreType.DMA((1,)),
            pltpu.SemaphoreType.DMA((1,)),
            pltpu.VMEM((rows, chunk), BF16),
            pltpu.VMEM((n_tp, rows, chunk), BF16),
            pltpu.SemaphoreType.DMA((1,)),
            pltpu.SemaphoreType.DMA((1,)),
            pltpu.SemaphoreType.DMA((1,)),
        ],
        compiler_params=pltpu.CompilerParams(
            collective_id=0, has_side_effects=True, vmem_limit_bytes=60 * 1024 * 1024
        ),
    )(*small, *large)


def shards(
    tokens,
    attn_gain,
    query_weight,
    key_weight,
    value_weight,
    forget_weight,
    forget_bias,
    cache_keys,
    cache_values,
    cache_gates,
    lengths,
    output_weight,
    ffn_gain,
    dense_gate_proj,
    dense_up_proj,
    dense_down_proj,
    dense_mix,
    expert_ids,
    group_prob,
    pair_prob,
    expert_gate,
    expert_up,
    expert_down,
):
    seq_count = tokens.shape[0]
    n_ep = lax.axis_size("ep")
    n_tp = lax.axis_size("tp")
    expert_count = n_ep * expert_gate.shape[0]
    capacity = max(4 * seq_count // expert_count, 8)
    model = (1, tokens.shape[1])
    return layer(
        n_ep,
        n_tp,
        capacity,
        (
            forget_bias.reshape(1, -1),
            lengths.reshape(1, -1),
            tokens,
            attn_gain.reshape(model),
            forget_weight.T,
            cache_gates,
            ffn_gain.reshape(n_ep // 2, 1, -1),
            dense_mix.reshape(-1, 128),
            expert_ids.T,
            group_prob.reshape(1, -1),
            pair_prob.T,
        ),
        (
            query_weight,
            key_weight,
            value_weight,
            output_weight,
            dense_gate_proj,
            dense_up_proj,
            dense_down_proj,
            cache_keys,
            cache_values,
            expert_gate.reshape(n_ep // 2, -1, expert_gate.shape[2]),
            expert_up.reshape(n_ep // 2, -1, expert_up.shape[2]),
            expert_down,
        ),
    )


def solution(mesh):
    return jax.shard_map(
        shards,
        mesh=mesh,
        in_specs=(
            P("ep", None),
            P(),
            P("ep", "tp"),
            P("ep", "tp"),
            P("ep", "tp"),
            P(None, "tp"),
            P("tp"),
            P("ep", "tp", None, None),
            P("ep", "tp", None, None),
            P("ep", "tp", None),
            P("ep"),
            P("tp", "ep"),
            P(),
            P("ep", "tp"),
            P("ep", "tp"),
            P("tp", "ep"),
            P(),
            P("ep", None),
            P("ep"),
            P("ep", None),
            P("ep", None, "tp"),
            P("ep", None, "tp"),
            P("ep", "tp", None),
        ),
        out_specs=P("ep", None),
        check_vma=False,
    )
```

```python
import functools
import math

import jax
import jax.numpy as jnp
from jax import lax
from jax.experimental import pallas as pl
from jax.experimental.pallas import tpu as pltpu
from jax.sharding import PartitionSpec as P

EPSILON = 1e-06


def rms_scale(values, norm_gain):
    widened = values.astype(jnp.float32)
    return (
        widened
        * lax.rsqrt(jnp.mean(widened * widened, axis=-1, keepdims=True) + EPSILON)
        * norm_gain
    )


MESH = pl.DeviceIdType.MESH
F32 = jnp.float32
BF16 = jnp.bfloat16


def flip(me, step):
    bit = 1
    while bit <= step:
        if step & bit:
            me = me + bit - 2 * bit * lax.rem(me // bit, 2)
        bit *= 2
    return me


def toward(me, step, count):
    return flip(me, step) if count & (count - 1) == 0 else lax.rem(me + step, count)


def origin(me, step, count):
    return flip(me, step) if count & (count - 1) == 0 else lax.rem(me + count - step, count)


def far_first(count):
    return range(count - 1, 0, -1)


def remote(source, place, send_sem, recv_sem, device):
    return pltpu.make_async_remote_copy(
        src_ref=source,
        dst_ref=place,
        send_sem=send_sem,
        recv_sem=recv_sem,
        device_id=device,
        device_id_type=MESH,
    )


def batch_of(landing, count, send_sem, recv_sem, device):
    blocks = landing.at[pl.ds(0, count)]
    return remote(blocks, blocks, send_sem.at[0], recv_sem.at[0], device)


def fan_out(axis, count, me, source_of, landing, send_sem, recv_sem):
    for step in far_first(count):
        target = toward(me, step, count)
        remote(
            source_of(target),
            landing.at[me],
            send_sem.at[0],
            recv_sem.at[0],
            {axis: target},
        ).start()
    return batch_of(landing, count - 1, send_sem, recv_sem, {axis: toward(me, 1, count)})


def arrive(axis, source, place, send_sem, recv_sem):
    remote(place, place, send_sem, recv_sem, {axis: source}).wait_recv()


def total_of(ref, count):
    total = ref[0].astype(F32)
    for index in range(1, count):
        total = total + ref[index].astype(F32)
    return total


def dot32(left, right):
    return jnp.dot(left, right, preferred_element_type=F32)


def silu(values):
    return values / (1.0 + jnp.exp(-values))


def chip_fan(axis, half, me, source_of, landing, send_sem, recv_sem):
    chip, core = me // 2, lax.rem(me, 2)
    for step in far_first(half):
        target = toward(chip, step, half)
        remote(
            source_of(target),
            landing.at[chip],
            send_sem.at[0],
            recv_sem.at[0],
            {axis: target * 2 + core},
        ).start()
    return batch_of(
        landing, half - 1, send_sem, recv_sem, {axis: toward(chip, 1, half) * 2 + core}
    )


def pick(one_hot, held):
    return lax.dot_general(
        one_hot, held, (((0,), (0,)), ((), ())), preferred_element_type=F32
    )


def slot_tables(ids, experts, slots):
    rows = ids.shape[1]
    row_at = lax.broadcasted_iota(jnp.int32, (rows, rows), 0)
    row_to = lax.broadcasted_iota(jnp.int32, (rows, rows), 1)
    expert_at = lax.broadcasted_iota(jnp.int32, (experts, rows), 0).astype(F32)
    slot_at = lax.broadcasted_iota(jnp.int32, (slots, rows), 0).astype(F32)
    first = ids[0:1, :] == expert_at
    second = ids[1:2, :] == expert_at
    hits = (first | second).astype(F32).astype(BF16)
    earlier = (row_at < row_to).astype(F32).astype(BF16)
    ranks = dot32(hits, earlier)
    tables = []
    for chosen in (first, second):
        place = jnp.where(chosen, ranks, -1.0)
        tables.append(
            jnp.concatenate(
                [
                    (place[expert : expert + 1, :] == slot_at).astype(F32)
                    for expert in range(experts)
                ],
                axis=0,
            )
        )
    return tables


def route_columns(group_prob, pair_prob):
    rows = pair_prob.shape[1]
    row_at = lax.broadcasted_iota(jnp.int32, (rows, rows), 0)
    row_to = lax.broadcasted_iota(jnp.int32, (rows, rows), 1)
    probs = pair_prob[...]
    shares = group_prob[...] * probs / (probs[0:1, :] + probs[1:2, :])
    return [
        jnp.sum(jnp.where(row_at == row_to, shares[k : k + 1, :], 0.0), axis=-1, keepdims=True)
        for k in range(2)
    ]


def layer_kernel(
    n_ep,
    n_tp,
    forget_bias_in,
    lengths_in,
    tokens_in,
    attn_gain_in,
    forget_rows_in,
    gates_in,
    gain_parts_in,
    dense_mix_in,
    expert_ids_in,
    group_prob_in,
    pair_prob_in,
    query_weight,
    key_weight,
    value_weight,
    output_weight,
    dense_gate,
    dense_up,
    dense_down,
    keys,
    values,
    expert_gate,
    expert_up,
    expert_down,
    out,
    forget_bias,
    lengths,
    tokens,
    attn_gain,
    forget_rows,
    gates,
    gain_parts,
    dense_mix,
    expert_ids,
    group_prob,
    pair_prob,
    small_sem,
    wide_held,
    tall_held,
    keys_held,
    values_held,
    expert_gate_held,
    expert_up_held,
    expert_down_held,
    load_sem,
    weight_ss,
    weight_rs,
    norm_send,
    norm_land,
    norm_ss,
    norm_rs,
    ids_send,
    ids_land,
    ids_ss,
    ids_rs,
    token_send,
    token_land,
    token_ss,
    token_rs,
    part_kept,
    part_send,
    part_land,
    part_ss,
    part_rs,
    query_flat,
    key_flat,
    value_flat,
    forget_flat,
    gate_flat,
    scores,
    mixed,
    attended,
    att_land,
    att_ss,
    att_rs,
    head_send,
    head_land,
    head_ss,
    head_rs,
    res_send,
    res_land,
    res_ss,
    res_rs,
    own_land,
    own_ss,
    own_rs,
    slot_send,
    slot_land,
    slot_ss,
    slot_rs,
    pass_ss,
    pass_rs,
    mix_parts,
    dense_send,
    dense_land,
    dense_ss,
    dense_rs,
    hidden_land,
    hidden_send,
    hidden_ss,
    hidden_rs,
    expert_send,
    expert_land,
    expert_ss,
    expert_rs,
    back_send,
    back_land,
    back_ss,
    back_rs,
    tail_send,
    tail_land,
    tail_ss,
    tail_rs,
    out_send,
    out_land,
    out_ss,
    out_rs,
):
    me = lax.axis_index("ep")
    me_tp = lax.axis_index("tp")
    barrier = pltpu.get_barrier_semaphore()
    half = n_ep // 2
    chip, core = me // 2, lax.rem(me, 2)
    spreads = chip == me_tp

    def greet(axis, mine, count):
        def signal(step, carry):
            pl.semaphore_signal(
                barrier,
                inc=1,
                device_id={axis: lax.rem(mine + step, count)},
                device_id_type=MESH,
            )
            return carry

        lax.fori_loop(1, count, signal, 0, unroll=count <= 8)

    greet("ep", me, n_ep)
    greet("tp", me_tp, n_tp)
    small_loads = [
        pltpu.make_async_copy(source, place, small_sem.at[index])
        for index, (source, place) in enumerate(
            (
                (tokens_in, tokens),
                (attn_gain_in, attn_gain),
                (expert_ids_in, expert_ids),
                (forget_bias_in, forget_bias),
                (forget_rows_in, forget_rows),
                (group_prob_in, group_prob),
                (pair_prob_in, pair_prob),
                (dense_mix_in, dense_mix),
                (gain_parts_in, gain_parts),
                (lengths_in, lengths),
                (gates_in, gates),
            )
        )
    ]
    for small in small_loads:
        small.start()
    rows, model = tokens.shape
    depth, hidden = query_weight.shape
    heads, span, size = keys.shape[1:]
    slots = slot_send.shape[1]
    chunk = model // n_tp
    cols = 2 * depth
    wide = 2 * hidden
    loads = [
        pltpu.make_async_copy(source, place, load_sem.at[index])
        for source, place, index in (
            (query_weight, wide_held.at[core, 0], 0),
            (key_weight, wide_held.at[core, 1], 0),
            (value_weight, wide_held.at[core, 2], 0),
            (dense_gate, wide_held.at[core, 3], 0),
            (dense_up, wide_held.at[core, 4], 0),
            (output_weight, tall_held.at[core, 0], 1),
            (dense_down, tall_held.at[core, 1], 1),
            (keys, keys_held, 2),
            (values, values_held, 3),
            (expert_gate, expert_gate_held, 4),
            (expert_up, expert_up_held, 5),
        )
    ]
    loads += [
        pltpu.make_async_copy(
            expert_down.at[0, :, pl.ds(index * chunk, chunk)],
            expert_down_held.at[index],
            load_sem.at[6],
        )
        for index in range(n_tp)
    ]
    for load in loads[:7]:
        load.start()

    def loaded(place, index):
        pltpu.make_async_copy(place, place, load_sem.at[index]).wait()

    gifts = [
        remote(
            place,
            place,
            weight_ss.at[index],
            weight_rs.at[index],
            {"ep": me + 1 - 2 * core},
        )
        for index, place in enumerate(
            (
                wide_held.at[core, pl.ds(0, 3)],
                wide_held.at[core, pl.ds(3, 2)],
                tall_held.at[core],
            )
        )
    ]

    for small in small_loads[:3]:
        small.wait()
    normed = rms_scale(tokens[...], attn_gain[...])
    for index in range(half):
        norm_send[index] = normed[:, index * cols : (index + 1) * cols].astype(BF16)
        token_send[index] = tokens[:, index * cols : (index + 1) * cols]
    ids = expert_ids[...].astype(F32)
    ids_send[0, 0:2, 0:rows] = ids
    pl.semaphore_wait(barrier, n_ep + n_tp - 2)

    norm_batch = chip_fan("ep", half, me, lambda t: norm_send.at[t], norm_land, norm_ss, norm_rs)
    sent = [norm_batch]
    norm_land[chip] = norm_send[chip]
    loaded(wide_held.at[core], 0)
    gifts[0].start()
    gifts[1].start()
    for load in loads[7:]:
        load.start()
    loaded(tall_held.at[core], 1)
    gifts[2].start()

    def row_copies(source_of, landing, send_sem, recv_sem):
        return [
            remote(
                source_of(toward(chip, step, half)),
                landing,
                send_sem.at[0],
                recv_sem.at[0],
                {"ep": toward(chip, step, half) * 2 + core},
            )
            for step in far_first(half)
        ]

    def row_arrival(landing, send_sem, recv_sem):
        @pl.when(jnp.logical_not(spreads))
        def _():
            arrive("ep", me_tp * 2 + core, landing, send_sem.at[0], recv_sem.at[0])

    def row_batch(blocks, send_sem, recv_sem):
        other = {"ep": toward(chip, 1, half) * 2 + core}
        return batch_of(blocks, half - 1, send_sem, recv_sem, other)

    spread_early = row_copies(lambda t: token_send.at[t], token_land, token_ss, token_rs)
    spread_early += row_copies(lambda t: ids_send.at[0], ids_land.at[0], ids_ss, ids_rs)

    @pl.when(spreads)
    def _():
        for copy in spread_early:
            copy.start()
        token_land[...] = token_send[chip]
        ids_land[0] = ids_send[0]

    norm_batch.wait_recv()
    gifts[0].wait_recv()
    joined = norm_land[...].reshape(half * rows, cols)
    part_batches = []
    for index in range(3):
        product = dot32(joined, wide_held[:, index].reshape(cols, hidden)).reshape(
            half, rows, hidden
        )
        part_send[index] = product.astype(BF16)
        part_batches.append(
            chip_fan(
                "ep",
                half,
                me,
                lambda t: part_send.at[index, t],
                part_land.at[index],
                part_ss.at[index],
                part_rs.at[index],
            )
        )
        part_kept[index] = product
    sent += part_batches
    for small in small_loads[3:]:
        small.wait()
    normed_wide = normed.astype(BF16).astype(F32)
    for head in range(heads):
        logit = forget_bias[0, head] + jnp.sum(
            normed_wide * forget_rows[head : head + 1, :].astype(F32), axis=-1, keepdims=True
        )
        forget_log = jnp.minimum(logit, 0.0) - jnp.log1p(jnp.exp(-jnp.abs(logit)))
        block = slice(head * rows, (head + 1) * rows)
        forget_flat[block, :] = jnp.broadcast_to(forget_log, (rows, size))
        gate_flat[block, :] = gates[:, head, :]
    mix_lanes = dense_mix.shape[1]
    mix_wide = dense_mix[...].astype(F32)
    for at in range(0, model, mix_lanes):
        start = at % cols
        mix_parts[at // cols, :, start : start + mix_lanes] = mix_wide[
            at // mix_lanes : at // mix_lanes + 1, :
        ]
    first_table, second_table = slot_tables(ids, n_ep, slots)
    to_first, to_second = first_table.astype(BF16), second_table.astype(BF16)
    first_route, second_route = route_columns(group_prob, pair_prob)
    row_arrival(ids_land.at[0], ids_ss, ids_rs)
    tables = slot_tables(ids_land[0][0:2, 0:rows], n_ep, slots)
    dispatch = (tables[0] + tables[1]).astype(BF16)
    row_arrival(token_land, token_ss, token_rs)

    def reduced(index, place):
        part_batches[index].wait_recv()
        total = part_kept[index, chip]
        for step in range(1, half):
            total = total + part_land[index, origin(chip, step, half)].astype(F32)
        total = total.astype(BF16).astype(F32)
        for head in range(heads):
            place[head * rows : (head + 1) * rows, :] = total[:, head * size : (head + 1) * size]

    flat = heads * rows
    scale = 1.0 / math.sqrt(size)
    positions = lax.broadcasted_iota(jnp.int32, (flat, span), 1)
    sequences = lax.broadcasted_iota(jnp.int32, (rows, size), 0)
    live_wide = jnp.zeros((rows, size), jnp.int32)
    for seq in range(rows):
        live_wide = jnp.where(sequences == seq, lengths[0, seq], live_wide)
    lives = jnp.concatenate([live_wide] * heads, axis=0)[:, 0:1]
    gate_all = gate_flat[...]
    last_gate = jnp.sum(jnp.where(positions == lives - 1, gate_all, 0.0), axis=-1, keepdims=True)
    gate_flat[...] = jnp.where(
        positions < lives, last_gate + forget_flat[:, 0:1] - gate_all, -jnp.inf
    )
    loaded(keys_held, 2)
    loaded(values_held, 3)
    reduced(0, query_flat)
    turned = jnp.transpose(query_flat[...]).astype(BF16)
    column = lax.broadcasted_iota(jnp.int32, (size, flat), 1)
    spots = [(head, seq) for head in range(heads) for seq in range(rows)]
    query_wide = jnp.concatenate(
        [
            jnp.where(column == spot, turned.astype(F32), 0.0).astype(BF16)
            for spot in range(flat)
        ],
        axis=0,
    )
    keys_wide = jnp.concatenate([keys_held[seq, head] for head, seq in spots], axis=1)
    score_all = jnp.transpose(dot32(keys_wide, query_wide)) * scale + gate_flat[...]
    reduced(1, key_flat)
    own_score = jnp.sum(query_flat[...] * key_flat[...], axis=-1, keepdims=True) * scale
    row_top = jnp.maximum(jnp.max(score_all, axis=-1, keepdims=True), own_score)
    raised = jnp.exp(score_all - row_top)
    own_raised = jnp.exp(own_score - row_top)
    totals = jnp.sum(raised, axis=-1, keepdims=True) + own_raised
    scores[...] = raised / totals
    own_prob = (own_raised / totals).astype(BF16).astype(F32)

    def value_step(seq, carry):
        for head in range(heads):
            line = pl.ds(head * rows + seq, 1)
            mixed[line, :] = dot32(scores[line, :].astype(BF16), values_held[seq, head])
        return carry

    lax.fori_loop(0, rows, value_step, 0, unroll=4)
    reduced(2, value_flat)
    blended = (mixed[...] + own_prob * value_flat[...]).astype(BF16)
    for head in range(heads):
        attended[:, head * size : (head + 1) * size] = blended[head * rows : (head + 1) * rows]

    att_batch = chip_fan("ep", half, me, lambda t: attended, att_land, att_ss, att_rs)
    att_land[chip] = attended[...]
    gifts[2].wait_recv()
    att_batch.wait_recv()
    joined = att_land[...].reshape(half * rows, hidden)
    for side in range(2):
        head_send[:, :, side * depth : (side + 1) * depth] = dot32(
            joined, tall_held[side, 0]
        ).reshape(n_tp, rows, depth)
    head_batch = fan_out(
        "tp", n_tp, me_tp, lambda t: head_send.at[t], head_land, head_ss, head_rs
    )
    head_batch.wait_recv()
    total = head_send[me_tp]
    for step in range(1, n_tp):
        total = total + head_land[origin(me_tp, step, n_tp)]
    residual = (token_land[...].astype(F32) + total).astype(BF16)
    res_send[...] = residual
    res_batch = fan_out("tp", n_tp, me_tp, lambda t: res_send, res_land, res_ss, res_rs)
    slot_send[...] = dot32(dispatch, residual).reshape(n_ep, slots, cols).astype(BF16)

    def slot_place(source):
        return slot_land.at[me_tp, source // 2, lax.rem(source, 2)]

    for step in far_first(n_ep):
        target = toward(me, step, n_ep)
        remote(
            slot_send.at[target],
            slot_place(me),
            slot_ss.at[0],
            slot_rs.at[me],
            {"ep": target},
        ).start()
    sent += [att_batch, head_batch, res_batch]
    sent.append(
        batch_of(slot_send, n_ep - 1, slot_ss, slot_rs, {"ep": toward(me, 1, n_ep)})
    )
    slot_land[me_tp, chip, core] = slot_send[me]
    res_land[me_tp] = residual

    def forward(source):
        for step in far_first(n_tp):
            remote(
                slot_place(source),
                slot_place(source),
                pass_ss.at[0],
                pass_rs.at[source // 2],
                {"tp": toward(me_tp, step, n_tp)},
            ).start()

    def relay(step):
        source = origin(me, step, n_ep)
        arrive("ep", source, slot_place(source), slot_ss.at[0], slot_rs.at[source])
        forward(source)

    forward(me)
    res_batch.wait_recv()
    gifts[1].wait_recv()
    held = res_land[...].reshape(half * rows, cols).astype(F32)
    dense_rows = (held * gain_parts[chip]).astype(BF16)
    for index in range(2):
        start = index * hidden
        dense_send[:, :, start : start + hidden] = (
            dot32(dense_rows, wide_held[:, 3 + index].reshape(cols, hidden))
            .reshape(half, rows, hidden)
            .astype(BF16)
        )
    squares = jnp.sum(held * held, axis=-1, keepdims=True)
    mixes = jnp.sum(dense_rows.astype(F32) * mix_parts[chip], axis=-1, keepdims=True)
    lane_at = lax.broadcasted_iota(jnp.int32, (half * rows, 128), 1)
    sums = jnp.where(lax.rem(lane_at, 2) == 0, squares, mixes)
    coarse = sums.astype(BF16).astype(F32)
    dense_send[:, :, wide:] = (
        jnp.where(lane_at < 2, coarse, sums - coarse).astype(BF16).reshape(half, rows, 128)
    )
    dense_batch = chip_fan(
        "ep", half, me, lambda t: dense_send.at[t], dense_land, dense_ss, dense_rs
    )
    dense_land[chip] = dense_send[chip]
    owner_copies = row_copies(lambda t: res_land.at[t], own_land, own_ss, own_rs)

    @pl.when(spreads)
    def _():
        for copy in owner_copies:
            copy.start()
        own_land[...] = res_land[chip]

    for step in range(1, n_ep):
        relay(step)

    def hidden_step():
        dense_batch.wait_recv()
        dense_sum = total_of(dense_land, half)
        sums = dense_sum[:, wide:]
        row_scale = lax.rsqrt((sums[:, 0:1] + sums[:, 2:3]) / model + EPSILON)
        mix = jax.nn.sigmoid((sums[:, 1:2] + sums[:, 3:4]) * row_scale)
        dense_pair = dense_sum[:, :wide] * row_scale
        hidden_send[...] = (silu(dense_pair[:, :hidden]) * dense_pair[:, hidden:]).astype(BF16)
        hidden_batch = chip_fan(
            "ep", half, me, lambda t: hidden_send, hidden_land, hidden_ss, hidden_rs
        )
        hidden_land[chip] = hidden_send[...]
        return mix, hidden_batch

    total_slots = n_ep * slots
    square = jnp.zeros((total_slots, cols), F32)
    gate_part = jnp.zeros((total_slots, hidden), F32)
    up_part = jnp.zeros((total_slots, hidden), F32)
    loaded(expert_gate_held, 4)
    loaded(expert_up_held, 5)
    for step in range(half):
        if step == half - 1:
            mix, hidden_batch = hidden_step()
        source = chip if step == 0 else origin(chip, step, half)
        blocks = slot_land.at[pl.ds(0, n_tp - 1), source]
        remote(
            blocks,
            blocks,
            pass_ss.at[0],
            pass_rs.at[source],
            {"tp": toward(me_tp, 1, n_tp)},
        ).wait_recv()
        part = slot_land[:, source].astype(F32).reshape(total_slots, cols)
        square = square + part * part
        part = (part * gain_parts[source]).astype(BF16)
        gate_part = gate_part + dot32(part, expert_gate_held[source])
        up_part = up_part + dot32(part, expert_up_held[source])
    slot_scale = lax.rsqrt(jnp.sum(square, axis=-1, keepdims=True) / model + EPSILON)
    expert_hidden = (silu(gate_part * slot_scale) * (up_part * slot_scale)).astype(BF16)

    loaded(expert_down_held, 6)
    for step in far_first(n_tp):
        target = toward(me_tp, step, n_tp)
        expert_send[target] = dot32(expert_hidden, expert_down_held[target]).astype(BF16)
        remote(
            expert_send.at[target],
            expert_land.at[me_tp],
            expert_ss.at[0],
            expert_rs.at[0],
            {"tp": target},
        ).start()
    expert_batch = batch_of(
        expert_land, n_tp - 1, expert_ss, expert_rs, {"tp": toward(me_tp, 1, n_tp)}
    )
    expert_land[me_tp] = dot32(expert_hidden, expert_down_held[me_tp]).astype(BF16)

    sent += [dense_batch, hidden_batch, expert_batch]

    hidden_batch.wait_recv()
    joined = hidden_land[...].reshape(half * rows, hidden)
    for side in range(2):
        tail_send[:, :, side * depth : (side + 1) * depth] = (
            dot32(joined, tall_held[side, 1]).reshape(half, rows, depth).astype(BF16)
        )

    def tail_copy(target):
        return remote(
            tail_send.at[target],
            tail_land.at[me_tp],
            tail_ss.at[0],
            tail_rs.at[0],
            {"ep": target * 2 + core, "tp": chip},
        )

    for step in range(half - 1, -1, -1):
        target = chip if step == 0 else toward(chip, step, half)
        if step:
            tail_copy(target).start()
        else:
            pl.when(jnp.logical_not(spreads))(lambda: tail_copy(chip).start())

    @pl.when(spreads)
    def _():
        tail_land[me_tp] = tail_send[chip]

    expert_batch.wait_recv()
    expert_total = total_of(expert_land, n_tp)
    for index in range(n_ep):
        back_send[index] = expert_total[index * slots : (index + 1) * slots].astype(BF16)
    back_batch = fan_out(
        "ep", n_ep, me, lambda t: back_send.at[t], back_land, back_ss, back_rs
    )
    back_land[me] = back_send[me]
    for copy in gifts:
        copy.wait_send()
    for copy in sent:
        copy.wait_send()
    passed = slot_land.at[pl.ds(0, n_tp - 1)]
    remote(
        passed, passed, pass_ss.at[0], pass_rs.at[0], {"tp": toward(me_tp, 1, n_tp)}
    ).wait_send()

    @pl.when(spreads)
    def _():
        row_batch(token_send, token_ss, token_rs).wait_send()
        row_batch(ids_send, ids_ss, ids_rs).wait_send()
        row_batch(res_land, own_ss, own_rs).wait_send()

    row_arrival(own_land, own_ss, own_rs)
    back_batch.wait_recv()
    back_rows = jnp.concatenate(
        [back_land[index].astype(F32) for index in range(n_ep)], axis=0
    ).astype(BF16)
    partial = (
        own_land[...].astype(F32)
        + first_route * pick(to_first, back_rows)
        + second_route * pick(to_second, back_rows)
    )
    def tail_batch(blocks, count):
        return batch_of(blocks, count, tail_ss, tail_rs, {"ep": toward(me, 2, n_ep)})

    for landed, count in ((spreads, half - 1), (jnp.logical_not(spreads), half)):

        @pl.when(landed)
        def _():
            tail_batch(tail_land, count).wait_recv()

    out_send[...] = (partial + mix * total_of(tail_land, n_tp)).astype(BF16)
    out_land[me_tp] = out_send[...]
    out_batch = fan_out("tp", n_tp, me_tp, lambda t: out_send, out_land, out_ss, out_rs)
    back_batch.wait_send()
    for left, count in ((spreads, half - 1), (jnp.logical_not(spreads), half)):

        @pl.when(left)
        def _():
            tail_batch(tail_send, count).wait_send()

    out_batch.wait_recv()
    for index in range(n_tp):
        out[:, index * chunk : (index + 1) * chunk] = out_land[index]
    out_batch.wait_send()


def layer(n_ep, n_tp, slots, small, large):
    rows, model = small[2].shape
    mix_shape = small[7].shape
    depth, hidden = large[0].shape
    keys = large[7]
    heads, span, size = keys.shape[1:]
    half = n_ep // 2
    chunk = model // n_tp
    cols = 2 * depth
    if half != n_tp:
        raise ValueError("unsupported mesh")
    hbm = pl.BlockSpec(memory_space=pltpu.HBM)
    return pl.pallas_call(
        functools.partial(layer_kernel, n_ep, n_tp),
        out_shape=pltpu.VMEM((rows, model), BF16),
        in_specs=[hbm] * (len(small) + len(large)),
        out_specs=pl.BlockSpec(memory_space=pltpu.VMEM),
        scratch_shapes=[
            pltpu.SMEM((1, heads), F32),
            pltpu.SMEM((1, rows), jnp.int32),
            pltpu.VMEM((rows, model), BF16),
            pltpu.VMEM((1, model), F32),
            pltpu.VMEM((heads, model), BF16),
            pltpu.VMEM((rows, heads, span), F32),
            pltpu.VMEM((half, 1, cols), F32),
            pltpu.VMEM(mix_shape, BF16),
            pltpu.VMEM((2, rows), jnp.int32),
            pltpu.VMEM((1, rows), F32),
            pltpu.VMEM((2, rows), F32),
            pltpu.SemaphoreType.DMA((11,)),
            pltpu.VMEM((2, 5, depth, hidden), BF16),
            pltpu.VMEM((2, 2, hidden, depth), BF16),
            pltpu.VMEM(keys.shape, BF16),
            pltpu.VMEM(keys.shape, BF16),
            pltpu.VMEM((half, cols, hidden), BF16),
            pltpu.VMEM((half, cols, hidden), BF16),
            pltpu.VMEM((n_tp, hidden, chunk), BF16),
            pltpu.SemaphoreType.DMA((7,)),
            pltpu.SemaphoreType.DMA((3,)),
            pltpu.SemaphoreType.DMA((3,)),
            pltpu.VMEM((half, rows, cols), BF16),
            pltpu.VMEM((half, rows, cols), BF16),
            pltpu.SemaphoreType.DMA((1,)),
            pltpu.SemaphoreType.DMA((1,)),
            pltpu.VMEM((half, 8, 128), F32),
            pltpu.VMEM((1, 8, 128), F32),
            pltpu.SemaphoreType.DMA((1,)),
            pltpu.SemaphoreType.DMA((1,)),
            pltpu.VMEM((half, rows, cols), BF16),
            pltpu.VMEM((rows, cols), BF16),
            pltpu.SemaphoreType.DMA((1,)),
            pltpu.SemaphoreType.DMA((1,)),
            pltpu.VMEM((3, half, rows, hidden), F32),
            pltpu.VMEM((3, half, rows, hidden), BF16),
            pltpu.VMEM((3, half, rows, hidden), BF16),
            pltpu.SemaphoreType.DMA((3, 1)),
            pltpu.SemaphoreType.DMA((3, 1)),
            pltpu.VMEM((heads * rows, size), F32),
            pltpu.VMEM((heads * rows, size), F32),
            pltpu.VMEM((heads * rows, size), F32),
            pltpu.VMEM((heads * rows, size), F32),
            pltpu.VMEM((heads * rows, span), F32),
            pltpu.VMEM((heads * rows, span), F32),
            pltpu.VMEM((heads * rows, size), F32),
            pltpu.VMEM((rows, hidden), BF16),
            pltpu.VMEM((half, rows, hidden), BF16),
            pltpu.SemaphoreType.DMA((1,)),
            pltpu.SemaphoreType.DMA((1,)),
            pltpu.VMEM((n_tp, rows, cols), F32),
            pltpu.VMEM((n_tp, rows, cols), F32),
            pltpu.SemaphoreType.DMA((1,)),
            pltpu.SemaphoreType.DMA((1,)),
            pltpu.VMEM((rows, cols), BF16),
            pltpu.VMEM((n_tp, rows, cols), BF16),
            pltpu.SemaphoreType.DMA((1,)),
            pltpu.SemaphoreType.DMA((1,)),
            pltpu.VMEM((rows, cols), BF16),
            pltpu.SemaphoreType.DMA((1,)),
            pltpu.SemaphoreType.DMA((1,)),
            pltpu.VMEM((n_ep, slots, cols), BF16),
            pltpu.VMEM((n_tp, half, 2, slots, cols), BF16),
            pltpu.SemaphoreType.DMA((1,)),
            pltpu.SemaphoreType.DMA((n_ep,)),
            pltpu.SemaphoreType.DMA((1,)),
            pltpu.SemaphoreType.DMA((half,)),
            pltpu.VMEM((half, 1, cols), F32),
            pltpu.VMEM((half, rows, 2 * hidden + 128), BF16),
            pltpu.VMEM((half, rows, 2 * hidden + 128), BF16),
            pltpu.SemaphoreType.DMA((1,)),
            pltpu.SemaphoreType.DMA((1,)),
            pltpu.VMEM((half, rows, hidden), BF16),
            pltpu.VMEM((rows, hidden), BF16),
            pltpu.SemaphoreType.DMA((1,)),
            pltpu.SemaphoreType.DMA((1,)),
            pltpu.VMEM((n_tp, n_ep * slots, chunk), BF16),
            pltpu.VMEM((n_tp, n_ep * slots, chunk), BF16),
            pltpu.SemaphoreType.DMA((1,)),
            pltpu.SemaphoreType.DMA((1,)),
            pltpu.VMEM((n_ep, slots, chunk), BF16),
            pltpu.VMEM((n_ep, slots, chunk), BF16),
            pltpu.SemaphoreType.DMA((1,)),
            pltpu.SemaphoreType.DMA((1,)),
            pltpu.VMEM((half, rows, cols), BF16),
            pltpu.VMEM((n_tp, rows, cols), BF16),
            pltpu.SemaphoreType.DMA((1,)),
            pltpu.SemaphoreType.DMA((1,)),
            pltpu.VMEM((rows, chunk), BF16),
            pltpu.VMEM((n_tp, rows, chunk), BF16),
            pltpu.SemaphoreType.DMA((1,)),
            pltpu.SemaphoreType.DMA((1,)),
        ],
        compiler_params=pltpu.CompilerParams(
            collective_id=0, has_side_effects=True, vmem_limit_bytes=60 * 1024 * 1024
        ),
    )(*small, *large)


def shards(
    tokens,
    attn_gain,
    query_weight,
    key_weight,
    value_weight,
    forget_weight,
    forget_bias,
    cache_keys,
    cache_values,
    cache_gates,
    lengths,
    output_weight,
    ffn_gain,
    dense_gate_proj,
    dense_up_proj,
    dense_down_proj,
    dense_mix,
    expert_ids,
    group_prob,
    pair_prob,
    expert_gate,
    expert_up,
    expert_down,
):
    seq_count = tokens.shape[0]
    n_ep = lax.axis_size("ep")
    n_tp = lax.axis_size("tp")
    expert_count = n_ep * expert_gate.shape[0]
    capacity = max(4 * seq_count // expert_count, 8)
    model = (1, tokens.shape[1])
    return layer(
        n_ep,
        n_tp,
        capacity,
        (
            forget_bias.reshape(1, -1),
            lengths.reshape(1, -1),
            tokens,
            attn_gain.reshape(model),
            forget_weight.T,
            cache_gates,
            ffn_gain.reshape(n_ep // 2, 1, -1),
            dense_mix.reshape(-1, 128),
            expert_ids.T,
            group_prob.reshape(1, -1),
            pair_prob.T,
        ),
        (
            query_weight,
            key_weight,
            value_weight,
            output_weight,
            dense_gate_proj,
            dense_up_proj,
            dense_down_proj,
            cache_keys,
            cache_values,
            expert_gate.reshape(n_ep // 2, -1, expert_gate.shape[2]),
            expert_up.reshape(n_ep // 2, -1, expert_up.shape[2]),
            expert_down,
        ),
    )


def solution(mesh):
    return jax.shard_map(
        shards,
        mesh=mesh,
        in_specs=(
            P("ep", None),
            P(),
            P("ep", "tp"),
            P("ep", "tp"),
            P("ep", "tp"),
            P(None, "tp"),
            P("tp"),
            P("ep", "tp", None, None),
            P("ep", "tp", None, None),
            P("ep", "tp", None),
            P("ep"),
            P("tp", "ep"),
            P(),
            P("ep", "tp"),
            P("ep", "tp"),
            P("tp", "ep"),
            P(),
            P("ep", None),
            P("ep"),
            P("ep", None),
            P("ep", None, "tp"),
            P("ep", None, "tp"),
            P("ep", "tp", None),
        ),
        out_specs=P("ep", None),
        check_vma=False,
    )
```
